32 devices in a mesh: ep: 8 (over z, x), tp: 4 (over y, core).
Axes of the slice: x: 2, y: 2, z: 4, core: 2. Of those that a mesh axis runs over, the one named last changes fastest.
Arguments:
- mix_input: bfloat16 [3072, 2048], P('ep', 'tp'), may hold values from -6 to 6
- mix_gain: float32 [2048], replicated, may hold values from 0.1 to 1.9
- gate_b_weight: bfloat16 [2048, 2048], P(None, 'tp'), may hold values from -0.125 to 0.125
- gate_c_weight: bfloat16 [2048, 2048], P(None, 'tp'), may hold values from -0.125 to 0.125
- value_weight: bfloat16 [2048, 2048], P(None, 'tp'), may hold values from -0.125 to 0.125
- conv_weight: float32 [3, 2048], P(None, 'tp'), may hold values from -3 to 3
- out_weight: bfloat16 [2048, 2048], P('tp'), may hold values from -0.125 to 0.125
- expert_input: bfloat16 [1280, 2048], P('ep', 'tp'), may hold values from -6 to 6
- expert_gain: float32 [2048], replicated, may hold values from 0.1 to 1.9
- routes: int32 [1280, 2], P('ep'), may hold values from 0 to 7, all different within a row; in each aligned block of 160 rows (0 to 159, 160 to 319, ...) at most 80 rows name the same one
- route_weight: float32 [1280, 2], P('ep'), may hold values from 0.2 to 1
- expert_gate: bfloat16 [8, 2048, 3072], P('ep', None, 'tp'), may hold values from -0.125 to 0.125
- expert_up: bfloat16 [8, 2048, 3072], P('ep', None, 'tp'), may hold values from -0.125 to 0.125
- expert_down: bfloat16 [8, 3072, 2048], P('ep', 'tp'), may hold values from -0.109375 to 0.109375
Outputs:
- mix_output: bfloat16 [3072, 2048], P('ep', 'tp')
- expert_output: bfloat16 [1280, 2048], P('ep', 'tp')
The draws below stay inside these ranges and needn't reach their ends.
Inputs may be any that keep to these rules, and one draw needn't show every extreme that they name: `routes`: the 2 experts of a row differ. Among the rows of one device no expert is named more than 80 times, a bound that some block reaches.
All inputs are finite; a program needn't handle non-finite values.
Results may differ from the reference program's by a relative error of at most 0.019.
Values may be sent and summed in bfloat16 or wider, within the bound.
A program may use at most 64 MiB of HBM per device.

```python
import math
import jax
import jax.numpy as jnp
import numpy as np
from jax import lax

D = 2048
FF = 3072
TOPK = 2
TOK_B = 160
EXPERTS = 8
CAP = 80
TOKENS_A = 3072
TOKENS_B = 1280
N_EP = 8
N_TP = 4


def levels(own_key, dims, split, low, high):
    def one(position, parts):
        draws = jax.random.uniform(jax.random.fold_in(jax.random.fold_in(own_key, 6), position), (parts,), jnp.float32, low / len(split), high / len(split))
        return jnp.repeat(jnp.exp(draws), dims[position] // parts).reshape((-1,) + (1,) * (len(dims) - position - 1))

    factor_of = one(*split[0])
    for cut in split[1:]:
        factor_of = factor_of * one(*cut)
    return factor_of


def shared_out(stream_key, own, number, rows, count, top, bound, slope):
    ranking = jax.random.permutation(stream_key, count)
    packed, common = load_shares(count, rows * top, bound, slope, True), load_shares(count, rows * top, bound, slope, False)
    places = jnp.arange(count)

    def named(tallies, rotation):
        used = int((tallies > 0).sum())
        fixed = max(1, used // 4)
        passed = fixed + (places - fixed + rotation * (used - fixed)) % max(1, count - fixed)
        return jnp.zeros((count,), jnp.int32).at[ranking[jnp.where(places < fixed, places, passed)]].set(jnp.asarray(tallies, jnp.int32))

    tallies = jnp.where(number % 4 == 0, named(packed, number // 4), named(common, number - number // 4 - 1))
    mixed = jax.random.permutation(jax.random.fold_in(own, 3), count)
    donor, receiver = mixed[0:count // 2 * 2:2], mixed[1:count // 2 * 2:2]
    margin = jnp.minimum(tallies[donor] - 1, bound - tallies[receiver]) // 2
    margin = jnp.where((donor == ranking[0]) | (receiver == ranking[0]) | (tallies[receiver] == 0), 0, jnp.maximum(margin, 0))
    passed = jax.random.randint(jax.random.fold_in(own, 4), (count // 2,), 0, 1 << 20) % (margin + 1)
    tallies = tallies.at[donor].add(-passed).at[receiver].add(passed)
    members = jnp.searchsorted(jnp.cumsum(tallies), jnp.arange(rows * top), side="right").astype(jnp.int32)
    listing = members.reshape(top, rows).T
    listing = listing[jax.random.permutation(jax.random.fold_in(own, 1), rows)]
    rotation = jax.random.randint(jax.random.fold_in(own, 2), (rows, 1), 0, top)
    return jnp.take_along_axis(listing, (jnp.arange(top)[None, :] + rotation) % top, axis=1)


def load_shares(number_of, total, bound, slope, full):
    weights = [(1 << 20) // math.isqrt(standing ** slope) + 1 for standing in range(1, number_of + 1)]
    largest = bound if full else min(bound, max(-(-total // number_of), total * weights[0] // sum(weights)))
    least = 1 if total - largest >= number_of - 1 else 0
    counts, rest = [largest] + [least] * (number_of - 1), total - largest - least * (number_of - 1)
    while rest > 0:
        candidates = [i for i in range(1, number_of) if counts[i] < largest] or [i for i in range(1, number_of) if counts[i] < bound]
        mass, left = sum([weights[i] for i in candidates]), rest
        for i in candidates:
            more = min(bound - counts[i], max(1, left * weights[i] // mass), rest)
            counts[i] = counts[i] + more
            rest = rest - more
    return np.array(counts)


def centred(own_key, shape, scale, reach, pieces=(), kind=jnp.bfloat16):
    drawn = scale * jax.random.normal(own_key, shape, jnp.float32)
    if pieces:
        drawn = drawn * levels(own_key, shape, pieces, -0.22, 0.18)
    return jnp.clip(drawn, -reach, reach).astype(kind)


def setup_inputs(seed: int = 0) -> dict:
    splits = jax.random.split(jax.random.key(seed), 15)
    mix_input = centred(splits[0], (TOKENS_A, D), 1.0, 6.0, ((0, 8), (1, 4)))
    mix_gain = jnp.clip(1.0 + 0.18 * jax.random.normal(splits[1], (D,), jnp.float32), 0.1, 1.9)
    gate_b_weight = centred(splits[2], (D, D), D ** -0.5, 0.125, ((1, 4),))
    gate_c_weight = centred(splits[3], (D, D), D ** -0.5, 0.125, ((1, 4),))
    value_weight = centred(splits[4], (D, D), D ** -0.5, 0.125, ((1, 4),))
    conv_weight = centred(splits[5], (3, D), 0.6, 3.0, ((1, 4),), jnp.float32)
    out_weight = centred(splits[6], (D, D), D ** -0.5, 0.125, ((0, 4),))
    expert_input = centred(splits[7], (TOKENS_B, D), 1.0, 6.0, ((0, 8), (1, 4)))
    expert_gain = jnp.clip(1.0 + 0.18 * jax.random.normal(splits[8], (D,), jnp.float32), 0.1, 1.9)
    routes_keys = jax.random.split(jax.random.fold_in(splits[9], 1), TOKENS_B // TOK_B)
    routes_turns = jax.random.permutation(jax.random.fold_in(splits[9], 3), TOKENS_B // TOK_B)
    routes = jax.vmap(lambda own, number: shared_out(jax.random.fold_in(splits[9], 2), own, number, TOK_B, EXPERTS, TOPK, CAP, 1))(routes_keys, routes_turns).reshape((TOKENS_B, TOPK))
    route_weight = jnp.clip(jnp.exp(math.log(1.0) - 1.609438 * jax.random.uniform(splits[10], (TOKENS_B, TOPK), jnp.float32) ** levels(splits[10], (TOKENS_B, TOPK), ((0, 8),), -0.2, 0.2)), 0.2, 1.0)
    expert_gate = centred(splits[11], (EXPERTS, D, FF), D ** -0.5, 0.125, ((0, 8), (2, 4)))
    expert_up = centred(splits[12], (EXPERTS, D, FF), D ** -0.5, 0.125, ((0, 8), (2, 4)))
    expert_down = centred(splits[13], (EXPERTS, FF, D), FF ** -0.5, 0.109375, ((0, 8), (1, 4)))
    return {"mix_input": mix_input, "mix_gain": mix_gain, "gate_b_weight": gate_b_weight, "gate_c_weight": gate_c_weight, "value_weight": value_weight, "conv_weight": conv_weight, "out_weight": out_weight, "expert_input": expert_input, "expert_gain": expert_gain, "routes": routes, "route_weight": route_weight, "expert_gate": expert_gate, "expert_up": expert_up, "expert_down": expert_down}


epsilon = 1e-06
routed_scale = 2.5

def norm_project(source, gain_vector, matrices):
    widened = source.astype(jnp.float32)
    factor = lax.rsqrt(lax.optimization_barrier(jnp.mean(widened * widened, axis=-1, keepdims=True)) + epsilon)
    scaled = (widened * gain_vector).astype(jnp.bfloat16)
    return [jnp.dot(scaled, matrix, preferred_element_type=jnp.float32) * factor for matrix in matrices]

def block_sum(operand, weights):
    span_size = operand.shape[1] // N_TP
    running = jnp.zeros((operand.shape[0], weights.shape[1]), jnp.float32)
    for block_index in range(N_TP):
        low = block_index * span_size
        partial_value = jnp.dot(operand[:, low:low + span_size], weights[low:low + span_size], preferred_element_type=jnp.float32)
        running = running + partial_value.astype(jnp.bfloat16).astype(jnp.float32)
    return running.astype(jnp.bfloat16)

def reference(mix_input, mix_gain, gate_b_weight, gate_c_weight, value_weight, conv_weight, out_weight, expert_input, expert_gain, routes, route_weight, expert_gate, expert_up, expert_down):
    outer_gate, inner_gate, conv_values = norm_project(mix_input, mix_gain, (gate_b_weight, gate_c_weight, value_weight))
    product = inner_gate * conv_values
    seq_length = product.shape[0]
    padded = jnp.concatenate([jnp.zeros((2, product.shape[1]), jnp.float32), product], axis=0)
    convolved = conv_weight[0] * padded[:seq_length] + conv_weight[1] * padded[1:seq_length + 1] + conv_weight[2] * padded[2:]
    gated = (outer_gate * convolved).astype(jnp.bfloat16)
    mix_output = block_sum(gated, out_weight)
    flat_routes = routes.reshape(-1).astype(jnp.int32)
    pair_count = flat_routes.shape[0]
    slot_count = N_EP * CAP
    expert_ids = jnp.arange(EXPERTS, dtype=jnp.int32)
    matches = (flat_routes[:, None] == expert_ids[None, :]).astype(jnp.int32)
    ranks = lax.optimization_barrier(jnp.sum((jnp.cumsum(matches, axis=0) - matches) * matches, axis=1)).astype(jnp.int32)
    owners_all = (jnp.arange(pair_count, dtype=jnp.int32) // TOPK).astype(jnp.int32)

    def one_expert(inputs):
        gate_matrix, up_matrix, down_matrix, expert_id = inputs
        chosen = flat_routes == expert_id
        target = jnp.where(chosen, ranks, slot_count).astype(jnp.int32)
        owners = jnp.zeros((slot_count,), jnp.int32).at[target].set(owners_all, mode='drop')
        gathered = expert_input[owners]
        hidden_gate, hidden_up = norm_project(gathered, expert_gain, (gate_matrix, up_matrix))
        activated = (jax.nn.silu(hidden_gate) * hidden_up).astype(jnp.bfloat16)
        return block_sum(activated, down_matrix)
    results = lax.map(one_expert, (expert_gate, expert_up, expert_down, expert_ids))
    picked = results[flat_routes, ranks].astype(jnp.float32).reshape(routes.shape[0], TOPK, -1)
    normalized = route_weight / lax.optimization_barrier(jnp.sum(route_weight, axis=1, keepdims=True)) * routed_scale
    expert_output = lax.optimization_barrier(jnp.sum(picked * normalized[:, :, None], axis=1)).astype(jnp.bfloat16)
    return (mix_output, expert_output)
```

```python
import functools

import jax
import jax.numpy as jnp
from jax import lax
from jax.experimental import pallas as pl
from jax.experimental.pallas import tpu as pltpu
from jax.sharding import PartitionSpec as P

MESH = pl.DeviceIdType.MESH
epsilon = 1e-06
routed_scale = 2.5
near = 4
f32 = jnp.float32
bf16 = jnp.bfloat16


def kernel(
    dims,
    mix_ref, mgain_ref, wb_hbm, wc_hbm, wv_hbm, conv_ref, wo_hbm,
    exp_ref, egain_ref, routes_ref, rw_ref, wg_hbm, wu_hbm, wd_hbm,
    mo_ref, eo_ref,
    wb, wc, wv, wo, wg, wu, wd, w_sem,
    gains, tables, outg,
    xg, xs, fac, outer, prod, edge, gated, pm, om, rm, sm, ym,
    xe, xes, efac, act, pe, oe, re, se, yr, fin, ra, rb, na, ny,
    mys, myr, mps, mpr, edges,
    eps, epr, eys, eyr, pps, ppr, hes, her, ses, ser, rts, rtr, nys, nyr,
    hms, hmr, yms, ymr,
):
    n_ep, n_tp, cap = dims
    chips = n_tp // 2
    n_blk = n_ep // near
    rows, feat = mix_ref.shape
    width = feat * n_tp
    half = feat * chips
    tok = exp_ref.shape[0]
    slots = n_ep * cap
    e = lax.axis_index("ep")
    t = lax.axis_index("tp")
    y, c = lax.div(t, 2), lax.rem(t, 2)
    partner = y * 2 + 1 - c
    blk, idx = lax.div(e, near), lax.rem(e, near)

    def source(p):
        return (
            lax.rem(blk + lax.div(p, near), n_blk) * near
            + lax.rem(idx + lax.rem(p, near), near)
        )

    def target(p):
        return (
            lax.rem(blk - lax.div(p, near) + n_blk, n_blk) * near
            + lax.rem(idx - lax.rem(p, near) + near, near)
        )

    def cols(b):
        return pl.ds(pl.multiple_of(b * feat, feat), feat)

    def lanes(k):
        return cols(c * chips + k)

    own_half = pl.ds(pl.multiple_of(c * half, half), half)

    def remote(src, dst, send_sem, recv_sem, ep, tp):
        return pltpu.make_async_remote_copy(
            src_ref=src, dst_ref=dst, send_sem=send_sem, recv_sem=recv_sem,
            device_id=(ep, tp), device_id_type=MESH,
        )

    def ahead(dy):
        return lax.rem(y + dy, chips)

    def peer(dy):
        return ahead(dy) * 2 + c

    def loop(first, last, body):
        lax.fori_loop(first, last, lambda i, carry: (body(i), carry)[1], 0)

    m_rows = rows // 2

    def mix_y(m, dy):
        at = pl.ds(m * m_rows, m_rows)
        return remote(
            mix_ref.at[at], xg.at[at, lanes(y)], mys.at[m, dy], myr.at[m, dy], e, peer(dy)
        )

    def mix_p(m):
        part = xg.at[pl.ds(m * m_rows, m_rows), own_half]
        return remote(part, part, mps.at[m], mpr.at[m], e, partner)

    def exp_out(p):
        return remote(outg.at[p], xe.at[p, :, lanes(y)], eps.at[p], epr.at[p], target(p), t)

    def exp_y(p, dy):
        part = xe.at[p, :, lanes(y)]
        return remote(part, part, eys.at[dy, p], eyr.at[dy, p], e, peer(dy))

    def exp_p(p):
        part = xe.at[p, :, own_half]
        return remote(part, part, pps.at[p], ppr.at[p], e, partner)

    def edge_copy():
        return remote(
            prod.at[pl.ds(rows, 8)], edge, edges.at[0], edges.at[1], lax.rem(e + 1, n_ep), t
        )

    def exp_half(j, first, last):
        at = pl.ds(first, last - first)
        return remote(pe.at[at], re.at[at], hes.at[j], her.at[j], e, partner)

    def exp_sum(p, dy):
        return remote(
            se.at[p, :, cols(ahead(dy))], yr.at[dy, p], ses.at[dy, p], ser.at[dy, p], e, peer(dy)
        )

    def near_back(p):
        return remote(se.at[p], ra.at[p], rts.at[p], rtr.at[p], source(p), t)

    def far_back(p):
        return remote(
            fin.at[p - near], rb.at[p - near], rts.at[p], rtr.at[p], source(p), t
        )

    def near_sum(dy):
        return remote(na.at[ahead(dy)], ny.at[dy], nys.at[dy], nyr.at[dy], e, peer(dy))

    def mix_half(q):
        return remote(pm.at[q], rm.at[q], hms.at[q], hmr.at[q], e, partner)

    def mix_sum(dy):
        return remote(sm.at[dy], ym.at[dy], yms.at[dy], ymr.at[dy], e, peer(dy))

    blocks = [(k, (k % chips) * 2 + k // chips) for k in range(n_tp)]

    def turned(src, dst, i):
        return [
            pltpu.make_async_copy(
                src.at[pl.ds(b * feat, feat)], dst.at[pl.ds(k * feat, feat)], w_sem.at[i, k]
            )
            for k, b in blocks
        ]

    loads = {
        "wg": turned(wg_hbm.at[0], wg, 0),
        "wu": turned(wu_hbm.at[0], wu, 1),
        "wd": [pltpu.make_async_copy(wd_hbm, wd, w_sem.at[2, 0])],
        "wc": turned(wc_hbm, wc, 3),
        "wv": turned(wv_hbm, wv, 4),
        "wb": turned(wb_hbm, wb, 5),
        "wo": [pltpu.make_async_copy(wo_hbm, wo, w_sem.at[6, 0])],
    }
    for group in loads.values():
        for load in group:
            load.start()

    def loaded(*names):
        for name in names:
            for load in loads[name]:
                load.wait()

    barrier = pltpu.get_barrier_semaphore()
    for dy in range(1, chips):
        pl.semaphore_signal(barrier, inc=1, device_id=(e, peer(dy)), device_id_type=MESH)
    pl.semaphore_signal(barrier, inc=1, device_id=(e, partner), device_id_type=MESH)

    def greet(d):
        pl.semaphore_signal(
            barrier, inc=1, device_id=(lax.rem(e + d, n_ep), t), device_id_type=MESH
        )

    loop(1, n_ep, greet)

    for k, b in blocks:
        to, at = pl.ds(k * feat, feat), pl.ds(b * feat, feat)
        gains[0:1, to] = mgain_ref[:, at]
        gains[1:2, to] = egain_ref[:, at]

    row = lax.broadcasted_iota(jnp.int32, (tok, tok), 0)
    column = lax.broadcasted_iota(jnp.int32, (tok, tok), 1)

    def upright(line):
        return jnp.sum(jnp.where(row == column, line, 0.0), axis=1, keepdims=True)

    lane_int = lax.broadcasted_iota(jnp.int32, (tok, 128), 1)
    lane = lane_int.astype(f32)
    first_slot = jnp.zeros((1, 128), f32)
    for p in range(n_ep):
        first_slot = first_slot + jnp.where(lane_int[0:1] == target(p), float(p * cap), 0.0)
    named = [upright(routes_ref[k : k + 1, :].astype(f32)) == lane for k in range(2)]
    either = jnp.where(named[0] | named[1], 1.0, 0.0).astype(bf16)
    before = row > column
    counts = jnp.dot(
        jnp.where(before, 1.0, 0.0).astype(bf16), either, preferred_element_type=f32
    )
    places = counts + first_slot
    slot_iota = lax.broadcasted_iota(jnp.int32, (tok, slots), 1).astype(f32)
    both = []
    for k in range(2):
        slot = jnp.sum(jnp.where(named[k], places, 0.0), axis=1, keepdims=True)
        one = jnp.where(slot_iota == slot, 1.0, 0.0)
        tables[k] = one.astype(bf16)
        both.append(one)
    send = (both[0] + both[1]).astype(bf16)

    outg[...] = (
        lax.dot_general(
            send, exp_ref[...], (((0,), (0,)), ((), ())), preferred_element_type=f32
        )
        .astype(bf16)
        .reshape(n_ep, cap, feat)
    )
    xe[0, :, lanes(y)] = outg[0]

    pl.semaphore_wait(barrier, n_ep - 1 + chips)

    middle = near + (n_ep - near) // 2
    parts = [(0, near), (near, middle), (middle, n_ep)]

    def pass_on(p):
        for dy in range(1, chips):
            exp_y(p, dy).start()

    def take(p):
        exp_out(p).wait_recv()
        pass_on(p)

    def relay(p):
        for dy in range(1, chips):
            exp_y(p, dy).wait_recv()
        exp_p(p).start()

    def mix_send(m):
        for dy in range(1, chips):
            mix_y(m, dy).start()

    def mix_relay(m):
        for dy in range(1, chips):
            mix_y(m, dy).wait_recv()
        mix_p(m).start()

    def scale_exp(p):
        at = pl.ds(pl.multiple_of(p * cap, cap), cap)
        exp_p(p).wait_recv()
        x = xe[p].astype(f32)
        efac[at] = lax.rsqrt(jnp.sum(x * x, axis=1, keepdims=True) / width + epsilon)
        xes[at] = (x * gains[1:2]).astype(bf16)

    hidden = wd.shape[0]
    wide_h = 256 if hidden % 256 == 0 else hidden

    def up(j):
        first, last = parts[j]
        part = pl.ds(first * cap, (last - first) * cap)
        loop(first, last, scale_exp)

        def activate(at):
            x = xes[part]
            factor = efac[part]
            gate = jnp.dot(x, wg[:, at], preferred_element_type=f32) * factor
            lift = jnp.dot(x, wu[:, at], preferred_element_type=f32) * factor
            act[part, at] = (gate / (1.0 + jnp.exp(-gate)) * lift).astype(bf16)

        if wide_h == hidden:
            activate(slice(None))
        else:
            loop(
                0, hidden // wide_h,
                lambda i: activate(pl.ds(pl.multiple_of(i * wide_h, wide_h), wide_h)),
            )

    def down(j):
        first, last = parts[j]
        part = pl.ds(first * cap, (last - first) * cap)

        def product(b, into, q):
            out = jnp.dot(act[part], wd[:, cols(b)], preferred_element_type=f32)
            into[pl.ds(first, last - first), :, cols(q)] = out.astype(bf16).reshape(
                last - first, cap, feat
            )

        loop(0, chips, lambda q: product(q * 2 + 1 - c, pe, q))
        exp_half(j, first, last).start()
        loop(0, chips, lambda q: product(q * 2 + c, oe, q))

    def joined(p, at):
        return oe[p, :, at].astype(f32) + re[p, :, at].astype(f32)

    def push_near(p):
        se[p] = joined(p, slice(None)).astype(bf16)

        @pl.when(p > 0)
        def _():
            near_back(p).start()

    def push_far(p):
        for dy in range(1, chips):
            at = cols(ahead(dy))
            se[p, :, at] = joined(p, at).astype(bf16)
            exp_sum(p, dy).start()

    def push(j):
        first, last = parts[j]
        exp_half(j, first, last).wait_recv()
        loop(first, last, push_near if first == 0 else push_far)

    def finish(p):
        whole = joined(p, cols(y))
        for dy in range(1, chips):
            exp_sum(p, dy).wait_recv()
            whole = whole + yr[dy, p].astype(f32)
        fin[p - near] = whole.astype(bf16)
        far_back(p).start()

    tile = 32

    def scale_mix(i):
        at = pl.ds(pl.multiple_of(i * tile, tile), tile)
        x = xg[at].astype(f32)
        fac[at] = lax.rsqrt(jnp.sum(x * x, axis=1, keepdims=True) / width + epsilon)
        xs[at] = (x * gains[0:1]).astype(bf16)

    wide = 256 if feat % 256 == 0 else feat

    def project(i):
        at = pl.ds(pl.multiple_of(i * wide, wide), wide)
        x = xs[...]
        factor = fac[...]
        inner = jnp.dot(x, wc[:, at], preferred_element_type=f32) * factor
        values = jnp.dot(x, wv[:, at], preferred_element_type=f32) * factor
        prod[pl.ds(8, rows), at] = inner * values
        outer[:, at] = jnp.dot(x, wb[:, at], preferred_element_type=f32) * factor

    def convolve(i):
        at = pl.ds(pl.multiple_of(i * 128, 128), 128)
        convolved = (
            conv_ref[0:1, at] * prod[pl.ds(6, rows), at]
            + conv_ref[1:2, at] * prod[pl.ds(7, rows), at]
            + conv_ref[2:3, at] * prod[pl.ds(8, rows), at]
        )
        gated[:, at] = (outer[:, at] * convolved).astype(bf16)

    def mix_down(b):
        return jnp.dot(gated[...], wo[:, cols(b)], preferred_element_type=f32).astype(bf16)

    def mix_given(q):
        pm[q] = mix_down(q * 2 + 1 - c)
        mix_half(q).start()

    def mix_kept(q):
        om[q] = mix_down(q * 2 + c)

    def mix_gates():
        for m in range(2):
            mix_p(m).wait_recv()
        loop(0, rows // tile, scale_mix)
        loaded("wc", "wv", "wb")
        loop(0, feat // wide, project)
        edge_copy().start()

    def mix_tail():
        edge_copy().wait_recv()
        prod[0:8] = jnp.where(e == 0, 0.0, edge[...])
        loop(0, feat // 128, convolve)
        loaded("wo")
        loop(0, chips, mix_given)
        loop(0, chips, mix_kept)
        for q in range(chips):
            mix_half(q).wait_recv()
        for dy in range(1, chips):
            q = ahead(dy)
            sm[dy] = (om[q].astype(f32) + rm[q].astype(f32)).astype(bf16)
            mix_sum(dy).start()

    loop(near, middle, lambda p: exp_out(p).start())
    loop(1, near, lambda p: exp_out(p).start())
    pass_on(0)
    mix_send(0)
    xg[:, lanes(y)] = mix_ref[...]
    loop(1, near, take)
    loop(near, middle, take)
    loop(middle, n_ep, lambda p: exp_out(p).start())
    mix_send(1)
    loop(0, near, relay)
    mix_relay(0)
    loaded("wg", "wu")
    up(0)
    loop(near, middle, relay)
    loaded("wd")
    down(0)
    loop(middle, n_ep, take)
    push(0)
    up(1)
    mix_relay(1)
    down(1)
    push(1)
    loop(middle, n_ep, relay)
    mix_gates()
    up(2)
    down(2)
    loop(near, middle, finish)
    push(2)
    mix_tail()
    loop(middle, n_ep, finish)

    scores = rw_ref[...]
    normalized = scores / jnp.sum(scores, axis=0, keepdims=True) * routed_scale
    share = [upright(normalized[k : k + 1, :]) for k in range(2)]

    def combine(first, last, results):
        return share[0] * jnp.dot(
            tables[0, :, first * cap : last * cap], results, preferred_element_type=f32
        ) + share[1] * jnp.dot(
            tables[1, :, first * cap : last * cap], results, preferred_element_type=f32
        )

    ra[0] = se[0]
    loop(1, near, lambda p: near_back(p).wait_recv())
    for q in range(chips):
        at = pl.ds(q * feat, feat)
        na[q] = combine(0, near, ra[:, :, at].reshape(near * cap, feat)).astype(bf16)
    for dy in range(1, chips):
        near_sum(dy).start()

    loop(near, n_ep, lambda p: far_back(p).wait_recv())
    result = combine(near, n_ep, rb[...].reshape(slots - near * cap, feat))
    result = result + na[y].astype(f32)
    for dy in range(1, chips):
        near_sum(dy).wait_recv()
        result = result + ny[dy].astype(f32)
    eo_ref[...] = result.astype(bf16)

    total = om[y].astype(f32) + rm[y].astype(f32)
    for dy in range(1, chips):
        mix_sum(dy).wait_recv()
        total = total + ym[dy].astype(f32)
    mo_ref[...] = total.astype(bf16)

    for dy in range(1, chips):
        near_sum(dy).wait_send()
        mix_sum(dy).wait_send()
        for m in range(2):
            mix_y(m, dy).wait_send()
    for m in range(2):
        mix_p(m).wait_send()
    edge_copy().wait_send()
    for q in range(chips):
        mix_half(q).wait_send()
    for j, (first, last) in enumerate(parts):
        exp_half(j, first, last).wait_send()

    def drain(p):
        exp_p(p).wait_send()
        for dy in range(1, chips):
            exp_y(p, dy).wait_send()

    def drain_out(p):
        exp_out(p).wait_send()

    def drain_far(p):
        far_back(p).wait_send()
        for dy in range(1, chips):
            exp_sum(p, dy).wait_send()

    loop(0, n_ep, drain)
    loop(1, n_ep, drain_out)
    loop(1, near, lambda p: near_back(p).wait_send())
    loop(near, n_ep, drain_far)


def solution(mesh):
    n_ep, n_tp = mesh.shape["ep"], mesh.shape["tp"]
    chips = n_tp // 2

    def local(
        mix_input, mix_gain, gate_b, gate_c, value_w, conv_weight, out_weight,
        expert_input, expert_gain, routes, route_weight, expert_gate, expert_up, expert_down,
    ):
        rows, feat = mix_input.shape
        width = feat * n_tp
        half = feat * chips
        tok, top = routes.shape
        experts = n_ep * expert_gate.shape[0]
        assert expert_gate.shape[0] == 1 and top == 2 and n_ep % near == 0
        cap = -(-(2 * tok * top // experts) // 16) * 16
        hidden = expert_gate.shape[2]
        slots = n_ep * cap
        far = n_ep - near
        vm, sem = pltpu.VMEM, pltpu.SemaphoreType.DMA
        scratch = [
            vm((width, feat), bf16), vm((width, feat), bf16), vm((width, feat), bf16),
            vm((feat, width), bf16),
            vm((width, hidden), bf16), vm((width, hidden), bf16), vm((hidden, width), bf16),
            sem((7, n_tp)),
            vm((2, width), f32), vm((2, tok, slots), bf16), vm((n_ep, cap, feat), bf16),
            vm((rows, width), bf16), vm((rows, width), bf16), vm((rows, 1), f32),
            vm((rows, feat), f32), vm((rows + 8, feat), f32), vm((8, feat), f32),
            vm((rows, feat), bf16),
            vm((chips, rows, feat), bf16), vm((chips, rows, feat), bf16),
            vm((chips, rows, feat), bf16), vm((chips, rows, feat), bf16),
            vm((chips, rows, feat), bf16),
            vm((n_ep, cap, width), bf16), vm((slots, width), bf16), vm((slots, 1), f32),
            vm((slots, hidden), bf16),
            vm((n_ep, cap, half), bf16), vm((n_ep, cap, half), bf16),
            vm((n_ep, cap, half), bf16), vm((n_ep, cap, half), bf16),
            vm((chips, n_ep, cap, feat), bf16), vm((far, cap, feat), bf16),
            vm((near, cap, half), bf16), vm((far, cap, feat), bf16),
            vm((chips, tok, feat), bf16), vm((chips, tok, feat), bf16),
            sem((2, chips)), sem((2, chips)), sem((2,)), sem((2,)), sem((2,)),
            sem((n_ep,)), sem((n_ep,)), sem((chips, n_ep)), sem((chips, n_ep)),
            sem((n_ep,)), sem((n_ep,)), sem((3,)), sem((3,)),
            sem((chips, n_ep)), sem((chips, n_ep)), sem((n_ep,)), sem((n_ep,)),
            sem((chips,)), sem((chips,)),
            sem((chips,)), sem((chips,)), sem((chips,)), sem((chips,)),
        ]
        v = pl.BlockSpec(memory_space=pltpu.VMEM)
        a = pl.BlockSpec(memory_space=pl.ANY)
        return pl.pallas_call(
            functools.partial(kernel, (n_ep, n_tp, cap)),
            out_shape=(
                jax.ShapeDtypeStruct((rows, feat), bf16),
                jax.ShapeDtypeStruct((tok, feat), bf16),
            ),
            in_specs=[v, v, a, a, a, v, a, v, v, v, v, a, a, a],
            out_specs=(v, v),
            scratch_shapes=scratch,
            compiler_params=pltpu.CompilerParams(
                collective_id=0, has_side_effects=True, vmem_limit_bytes=62 << 20
            ),
        )(
            mix_input, mix_gain.reshape(1, -1), gate_b, gate_c, value_w, conv_weight, out_weight,
            expert_input, expert_gain.reshape(1, -1), routes.T, route_weight.T,
            expert_gate, expert_up, expert_down.reshape(hidden, width),
        )

    in_specs = (
        P("ep", "tp"), P(), P(None, "tp"), P(None, "tp"), P(None, "tp"), P(None, "tp"),
        P("tp", None), P("ep", "tp"), P(), P("ep", None), P("ep", None),
        P("ep", None, "tp"), P("ep", None, "tp"), P("ep", "tp", None),
    )
    out_specs = (P("ep", "tp"), P("ep", "tp"))
    return jax.shard_map(local, mesh=mesh, in_specs=in_specs, out_specs=out_specs, check_vma=False)
```

```python
import functools

import jax
import jax.numpy as jnp
from jax import lax
from jax.experimental import pallas as pl
from jax.experimental.pallas import tpu as pltpu
from jax.sharding import PartitionSpec as P

MESH = pl.DeviceIdType.MESH
epsilon = 1e-06
routed_scale = 2.5
near = 4
f32 = jnp.float32
bf16 = jnp.bfloat16


def kernel(
    dims,
    mix_hbm, mgain_hbm, wb_hbm, wc_hbm, wv_hbm, conv_hbm, wo_hbm,
    exp_hbm, egain_hbm, routes_hbm, rw_hbm, wg_hbm, wu_hbm, wd_hbm,
    mo_hbm, eo_hbm,
    mix_ref, mgain_ref, conv_ref, exp_ref, egain_ref, routes_ref, rw_ref, mo_ref, eo_ref, i_sem,
    wb, wc, wv, wo, wg, wu, wd, w_sem,
    gains, tables, outg,
    xg, xs, fac, outer, prod, edge, gated, pm, om, rm, sm, ym,
    xe, xes, efac, act, pe, oe, re, se, yr, fin, ra, rb, na, ny,
    mys, myr, mps, mpr, edges,
    eps, epr, eys, eyr, pps, ppr, hes, her, ses, ser, rts, rtr, nys, nyr,
    hms, hmr, yms, ymr,
):
    n_ep, n_tp, cap = dims
    chips = n_tp // 2
    n_blk = n_ep // near
    rows, feat = mix_ref.shape
    width = feat * n_tp
    half = feat * chips
    tok = exp_ref.shape[0]
    slots = n_ep * cap
    e = lax.axis_index("ep")
    t = lax.axis_index("tp")
    y, c = lax.div(t, 2), lax.rem(t, 2)
    partner = y * 2 + 1 - c
    blk, idx = lax.div(e, near), lax.rem(e, near)

    def source(p):
        return (
            lax.rem(blk + lax.div(p, near), n_blk) * near
            + lax.rem(idx + lax.rem(p, near), near)
        )

    def target(p):
        return (
            lax.rem(blk - lax.div(p, near) + n_blk, n_blk) * near
            + lax.rem(idx - lax.rem(p, near) + near, near)
        )

    def cols(b):
        return pl.ds(pl.multiple_of(b * feat, feat), feat)

    def lanes(k):
        return cols(c * chips + k)

    own_half = pl.ds(pl.multiple_of(c * half, half), half)

    def remote(src, dst, send_sem, recv_sem, ep, tp):
        return pltpu.make_async_remote_copy(
            src_ref=src, dst_ref=dst, send_sem=send_sem, recv_sem=recv_sem,
            device_id=(ep, tp), device_id_type=MESH,
        )

    def ahead(dy):
        return lax.rem(y + dy, chips)

    def peer(dy):
        return ahead(dy) * 2 + c

    def loop(first, last, body):
        lax.fori_loop(first, last, lambda i, carry: (body(i), carry)[1], 0)

    m_rows = rows // 2

    def mix_y(m, dy):
        at = pl.ds(m * m_rows, m_rows)
        return remote(
            mix_ref.at[at], xg.at[at, lanes(y)], mys.at[m, dy], myr.at[m, dy], e, peer(dy)
        )

    def mix_p(m):
        part = xg.at[pl.ds(m * m_rows, m_rows), own_half]
        return remote(part, part, mps.at[m], mpr.at[m], e, partner)

    def exp_out(p):
        return remote(outg.at[p], xe.at[p, :, lanes(y)], eps.at[p], epr.at[p], target(p), t)

    def exp_y(p, dy):
        part = xe.at[p, :, lanes(y)]
        return remote(part, part, eys.at[dy, p], eyr.at[dy, p], e, peer(dy))

    def exp_p(p):
        part = xe.at[p, :, own_half]
        return remote(part, part, pps.at[p], ppr.at[p], e, partner)

    def edge_copy():
        return remote(
            prod.at[pl.ds(rows, 8)], edge, edges.at[0], edges.at[1], lax.rem(e + 1, n_ep), t
        )

    def exp_half(j, first, last):
        at = pl.ds(first, last - first)
        return remote(pe.at[at], re.at[at], hes.at[j], her.at[j], e, partner)

    def exp_sum(p, dy):
        return remote(
            se.at[p, :, cols(ahead(dy))], yr.at[dy, p], ses.at[dy, p], ser.at[dy, p], e, peer(dy)
        )

    def near_back(p):
        return remote(se.at[p], ra.at[p], rts.at[p], rtr.at[p], source(p), t)

    def far_back(p):
        return remote(
            fin.at[p - near], rb.at[p - near], rts.at[p], rtr.at[p], source(p), t
        )

    def near_sum(dy):
        return remote(na.at[ahead(dy)], ny.at[dy], nys.at[dy], nyr.at[dy], e, peer(dy))

    def mix_half(q):
        return remote(pm.at[q], rm.at[q], hms.at[q], hmr.at[q], e, partner)

    def mix_sum(dy):
        return remote(sm.at[dy], ym.at[dy], yms.at[dy], ymr.at[dy], e, peer(dy))

    barrier = pltpu.get_barrier_semaphore()
    for dy in range(1, chips):
        pl.semaphore_signal(barrier, inc=1, device_id=(e, peer(dy)), device_id_type=MESH)
    pl.semaphore_signal(barrier, inc=1, device_id=(e, partner), device_id_type=MESH)

    def greet(d):
        pl.semaphore_signal(
            barrier, inc=1, device_id=(lax.rem(e + d, n_ep), t), device_id_type=MESH
        )

    loop(1, n_ep, greet)

    blocks = [(k, (k % chips) * 2 + k // chips) for k in range(n_tp)]

    def turned(src, dst, i):
        return [
            pltpu.make_async_copy(
                src.at[pl.ds(b * feat, feat)], dst.at[pl.ds(k * feat, feat)], w_sem.at[i, k]
            )
            for k, b in blocks
        ]

    loads = {
        "wg": turned(wg_hbm.at[0], wg, 0),
        "wu": turned(wu_hbm.at[0], wu, 1),
        "wd": [pltpu.make_async_copy(wd_hbm, wd, w_sem.at[2, 0])],
        "wc": turned(wc_hbm, wc, 3),
        "wv": turned(wv_hbm, wv, 4),
        "wb": turned(wb_hbm, wb, 5),
        "wo": [pltpu.make_async_copy(wo_hbm, wo, w_sem.at[6, 0])],
    }
    small = {
        name: pltpu.make_async_copy(src, dst, i_sem.at[i])
        for i, (name, src, dst) in enumerate(
            (
                ("routes", routes_hbm, routes_ref), ("exp", exp_hbm, exp_ref),
                ("mix", mix_hbm, mix_ref), ("mgain", mgain_hbm, mgain_ref),
                ("egain", egain_hbm, egain_ref), ("conv", conv_hbm, conv_ref),
                ("rw", rw_hbm, rw_ref),
            )
        )
    }
    for load in small.values():
        load.start()
    for load in small.values():
        load.wait()
    for group in loads.values():
        for load in group:
            load.start()

    def loaded(*names):
        for name in names:
            for load in loads[name]:
                load.wait()

    row = lax.broadcasted_iota(jnp.int32, (tok, tok), 0)
    column = lax.broadcasted_iota(jnp.int32, (tok, tok), 1)

    def upright(line):
        return jnp.sum(jnp.where(row == column, line, 0.0), axis=1, keepdims=True)

    lane_int = lax.broadcasted_iota(jnp.int32, (tok, 128), 1)
    lane = lane_int.astype(f32)
    first_slot = jnp.zeros((1, 128), f32)
    for p in range(n_ep):
        first_slot = first_slot + jnp.where(lane_int[0:1] == target(p), float(p * cap), 0.0)
    named = [upright(routes_ref[k : k + 1, :].astype(f32)) == lane for k in range(2)]
    either = jnp.where(named[0] | named[1], 1.0, 0.0).astype(bf16)
    before = row > column
    counts = jnp.dot(
        jnp.where(before, 1.0, 0.0).astype(bf16), either, preferred_element_type=f32
    )
    places = counts + first_slot
    slot_iota = lax.broadcasted_iota(jnp.int32, (tok, slots), 1).astype(f32)
    both = []
    for k in range(2):
        slot = jnp.sum(jnp.where(named[k], places, 0.0), axis=1, keepdims=True)
        one = jnp.where(slot_iota == slot, 1.0, 0.0)
        tables[k] = one.astype(bf16)
        both.append(one)
    send = (both[0] + both[1]).astype(bf16)

    outg[...] = (
        lax.dot_general(
            send, exp_ref[...], (((0,), (0,)), ((), ())), preferred_element_type=f32
        )
        .astype(bf16)
        .reshape(n_ep, cap, feat)
    )
    xe[0, :, lanes(y)] = outg[0]

    for k, b in blocks:
        to, at = pl.ds(k * feat, feat), pl.ds(b * feat, feat)
        gains[0:1, to] = mgain_ref[:, at]
        gains[1:2, to] = egain_ref[:, at]

    pl.semaphore_wait(barrier, n_ep - 1 + chips)

    middle = near + (n_ep - near) // 2
    parts = [(0, near), (near, middle), (middle, n_ep)]

    def pass_on(p):
        for dy in range(1, chips):
            exp_y(p, dy).start()

    def take(p):
        exp_out(p).wait_recv()
        pass_on(p)

    def relay(p):
        for dy in range(1, chips):
            exp_y(p, dy).wait_recv()
        exp_p(p).start()

    def mix_send(m):
        for dy in range(1, chips):
            mix_y(m, dy).start()

    def mix_sent(m):
        for dy in range(1, chips):
            mix_y(m, dy).wait_send()

    def mix_relay(m):
        for dy in range(1, chips):
            mix_y(m, dy).wait_recv()
        mix_p(m).start()

    def scale_exp(p):
        at = pl.ds(pl.multiple_of(p * cap, cap), cap)
        exp_p(p).wait_recv()
        x = xe[p].astype(f32)
        efac[at] = lax.rsqrt(jnp.sum(x * x, axis=1, keepdims=True) / width + epsilon)
        xes[at] = (x * gains[1:2]).astype(bf16)

    hidden = wd.shape[0]
    wide_h = 256 if hidden % 256 == 0 else hidden

    def scale(j):
        first, last = parts[j]
        loop(first, last, scale_exp)

    def up(j):
        first, last = parts[j]
        part = pl.ds(first * cap, (last - first) * cap)

        def activate(at):
            x = xes[part]
            factor = efac[part]
            gate = jnp.dot(x, wg[:, at], preferred_element_type=f32) * factor
            lift = jnp.dot(x, wu[:, at], preferred_element_type=f32) * factor
            act[part, at] = (gate / (1.0 + jnp.exp(-gate)) * lift).astype(bf16)

        if wide_h == hidden:
            activate(slice(None))
        else:
            loop(
                0, hidden // wide_h,
                lambda i: activate(pl.ds(pl.multiple_of(i * wide_h, wide_h), wide_h)),
            )

    def down(j):
        first, last = parts[j]
        part = pl.ds(first * cap, (last - first) * cap)

        def product(b, into, q):
            out = jnp.dot(act[part], wd[:, cols(b)], preferred_element_type=f32)
            into[pl.ds(first, last - first), :, cols(q)] = out.astype(bf16).reshape(
                last - first, cap, feat
            )

        loop(0, chips, lambda q: product(q * 2 + 1 - c, pe, q))
        exp_half(j, first, last).start()
        loop(0, chips, lambda q: product(q * 2 + c, oe, q))

    def joined(p, at):
        return oe[p, :, at].astype(f32) + re[p, :, at].astype(f32)

    def push_near(p):
        se[p] = joined(p, slice(None)).astype(bf16)

        @pl.when(p > 0)
        def _():
            near_back(p).start()

    def push_far(p):
        for dy in range(1, chips):
            at = cols(ahead(dy))
            se[p, :, at] = joined(p, at).astype(bf16)
            exp_sum(p, dy).start()

    def push(j):
        first, last = parts[j]
        exp_half(j, first, last).wait_recv()
        loop(first, last, push_near if first == 0 else push_far)

    def push_paced(j):
        first, last = parts[j]
        exp_half(j, first, last).wait_recv()
        push_far(first)
        for p in range(first + 1, last):
            for dy in range(1, chips):
                at = cols(ahead(dy))
                se[p, :, at] = joined(p, at).astype(bf16)
            for dy in range(1, chips):
                exp_sum(p - 1, dy).wait_send()
                exp_sum(p, dy).start()

    def finish(p):
        whole = joined(p, cols(y))
        for dy in range(1, chips):
            exp_sum(p, dy).wait_recv()
            whole = whole + yr[dy, p].astype(f32)
        fin[p - near] = whole.astype(bf16)
        far_back(p).start()

    tile = 32

    def scale_mix(i):
        at = pl.ds(pl.multiple_of(i * tile, tile), tile)
        x = xg[at].astype(f32)
        fac[at] = lax.rsqrt(jnp.sum(x * x, axis=1, keepdims=True) / width + epsilon)
        xs[at] = (x * gains[0:1]).astype(bf16)

    wide = 256 if feat % 256 == 0 else feat

    def project(m, i):
        at = pl.ds(pl.multiple_of(i * wide, wide), wide)
        part = pl.ds(m * m_rows, m_rows)
        x = xs[part]
        factor = fac[part]
        inner = jnp.dot(x, wc[:, at], preferred_element_type=f32) * factor
        values = jnp.dot(x, wv[:, at], preferred_element_type=f32) * factor
        prod[pl.ds(8 + m * m_rows, m_rows), at] = inner * values
        outer[part, at] = jnp.dot(x, wb[:, at], preferred_element_type=f32) * factor

    def convolve(i):
        at = pl.ds(pl.multiple_of(i * 128, 128), 128)
        convolved = (
            conv_ref[0:1, at] * prod[pl.ds(6, rows), at]
            + conv_ref[1:2, at] * prod[pl.ds(7, rows), at]
            + conv_ref[2:3, at] * prod[pl.ds(8, rows), at]
        )
        gated[:, at] = (outer[:, at] * convolved).astype(bf16)

    def mix_down(b):
        return jnp.dot(gated[...], wo[:, cols(b)], preferred_element_type=f32).astype(bf16)

    def mix_given(q):
        pm[q] = mix_down(q * 2 + 1 - c)
        mix_half(q).start()

    def mix_kept(q):
        om[q] = mix_down(q * 2 + c)

    def mix_scale(m):
        mix_p(m).wait_recv()
        loop(m * m_rows // tile, (m + 1) * m_rows // tile, scale_mix)

    def mix_gates(m):
        loop(0, feat // wide, lambda i: project(m, i))

    def mix_conv():
        edge_copy().wait_recv()
        prod[0:8] = jnp.where(e == 0, 0.0, edge[...])
        loop(0, feat // 128, convolve)
        loaded("wo")

    def mix_dots():
        loop(0, chips, mix_given)
        loop(0, chips, mix_kept)

    def mix_push():
        for q in range(chips):
            mix_half(q).wait_recv()
        for dy in range(1, chips):
            q = ahead(dy)
            sm[dy] = (om[q].astype(f32) + rm[q].astype(f32)).astype(bf16)
            mix_sum(dy).start()

    loop(near, middle, lambda p: exp_out(p).start())
    loop(1, near, lambda p: exp_out(p).start())
    mix_send(0)
    xg[:, lanes(y)] = mix_ref[...]
    mix_sent(0)
    loop(middle, n_ep, lambda p: exp_out(p).start())
    mix_send(1)
    mix_relay(0)
    mix_scale(0)
    loop(near, middle, take)
    loaded("wc", "wv", "wb")
    mix_gates(0)
    mix_relay(1)
    loop(1, near, take)
    pass_on(0)
    mix_scale(1)
    mix_gates(1)
    edge_copy().start()
    loop(near, middle, relay)
    loaded("wg", "wu")
    scale(1)
    up(1)
    loop(middle, n_ep, take)
    loaded("wd")
    down(1)
    mix_conv()
    push(1)
    mix_dots()
    loop(0, near, relay)
    scale(0)
    mix_push()
    up(0)
    loop(middle, n_ep, relay)
    down(0)
    loop(near, middle, finish)
    scale(2)
    push(0)
    up(2)
    down(2)
    push(2)
    loop(middle, n_ep, finish)

    scores = rw_ref[...]
    normalized = scores / jnp.sum(scores, axis=0, keepdims=True) * routed_scale
    share = [upright(normalized[k : k + 1, :]) for k in range(2)]

    def combine(first, last, results):
        return share[0] * jnp.dot(
            tables[0, :, first * cap : last * cap], results, preferred_element_type=f32
        ) + share[1] * jnp.dot(
            tables[1, :, first * cap : last * cap], results, preferred_element_type=f32
        )

    ra[0] = se[0]
    loop(1, near, lambda p: near_back(p).wait_recv())
    for q in range(chips):
        at = pl.ds(q * feat, feat)
        na[q] = combine(0, near, ra[:, :, at].reshape(near * cap, feat)).astype(bf16)
    for dy in range(1, chips):
        near_sum(dy).start()

    total = om[y].astype(f32) + rm[y].astype(f32)
    for dy in range(1, chips):
        mix_sum(dy).wait_recv()
        total = total + ym[dy].astype(f32)
    mo_ref[...] = total.astype(bf16)
    mo_out = pltpu.make_async_copy(mo_ref, mo_hbm, i_sem.at[7])
    mo_out.start()

    loop(near, n_ep, lambda p: far_back(p).wait_recv())
    result = combine(near, n_ep, rb[...].reshape(slots - near * cap, feat))
    result = result + na[y].astype(f32)
    for dy in range(1, chips):
        near_sum(dy).wait_recv()
        result = result + ny[dy].astype(f32)
    eo_ref[...] = result.astype(bf16)

    eo_out = pltpu.make_async_copy(eo_ref, eo_hbm, i_sem.at[8])
    eo_out.start()
    mo_out.wait()
    eo_out.wait()

    for dy in range(1, chips):
        near_sum(dy).wait_send()
        mix_sum(dy).wait_send()
        mix_y(1, dy).wait_send()
    for m in range(2):
        mix_p(m).wait_send()
    edge_copy().wait_send()
    for q in range(chips):
        mix_half(q).wait_send()
    for j, (first, last) in enumerate(parts):
        exp_half(j, first, last).wait_send()

    def drain(p):
        exp_p(p).wait_send()
        for dy in range(1, chips):
            exp_y(p, dy).wait_send()

    def drain_out(p):
        exp_out(p).wait_send()

    def drain_far(p):
        far_back(p).wait_send()

    def drain_sum(p):
        for dy in range(1, chips):
            exp_sum(p, dy).wait_send()

    loop(0, n_ep, drain)
    loop(1, n_ep, drain_out)
    loop(1, near, lambda p: near_back(p).wait_send())
    loop(near, n_ep, drain_far)
    loop(near, n_ep, drain_sum)


def hand_over(mix_hbm, exp_hbm, mo_hbm, eo_hbm, mix_vm, exp_vm, sems):
    pairs = ((exp_hbm, exp_vm, eo_hbm), (mix_hbm, mix_vm, mo_hbm))
    reads = [pltpu.make_async_copy(a, b, sems.at[0, i]) for i, (a, b, _) in enumerate(pairs)]
    writes = [pltpu.make_async_copy(b, d, sems.at[1, i]) for i, (_, b, d) in enumerate(pairs)]
    for read in reads:
        read.start()
    for read, write in zip(reads, writes):
        read.wait()
        write.start()
    for write in writes:
        write.wait()


def solution(mesh):
    n_ep, n_tp = mesh.shape["ep"], mesh.shape["tp"]
    chips = n_tp // 2

    def local(
        mix_input, mix_gain, gate_b, gate_c, value_w, conv_weight, out_weight,
        expert_input, expert_gain, routes, route_weight, expert_gate, expert_up, expert_down,
    ):
        rows, feat = mix_input.shape
        width = feat * n_tp
        half = feat * chips
        tok, top = routes.shape
        experts = n_ep * expert_gate.shape[0]
        assert expert_gate.shape[0] == 1 and top == 2 and n_ep % near == 0
        cap = -(-(2 * tok * top // experts) // 16) * 16
        hidden = expert_gate.shape[2]
        slots = n_ep * cap
        far = n_ep - near
        vm, sem = pltpu.VMEM, pltpu.SemaphoreType.DMA
        scratch = [
            vm((rows, feat), bf16), vm((1, width), f32), vm((3, feat), f32), vm((tok, feat), bf16),
            vm((1, width), f32), vm((2, tok), jnp.int32), vm((2, tok), f32),
            vm((rows, feat), bf16), vm((tok, feat), bf16), sem((9,)),
            vm((width, feat), bf16), vm((width, feat), bf16), vm((width, feat), bf16),
            vm((feat, width), bf16),
            vm((width, hidden), bf16), vm((width, hidden), bf16), vm((hidden, width), bf16),
            sem((7, n_tp)),
            vm((2, width), f32), vm((2, tok, slots), bf16), vm((n_ep, cap, feat), bf16),
            vm((rows, width), bf16), vm((rows, width), bf16), vm((rows, 1), f32),
            vm((rows, feat), f32), vm((rows + 8, feat), f32), vm((8, feat), f32),
            vm((rows, feat), bf16),
            vm((chips, rows, feat), bf16), vm((chips, rows, feat), bf16),
            vm((chips, rows, feat), bf16), vm((chips, rows, feat), bf16),
            vm((chips, rows, feat), bf16),
            vm((n_ep, cap, width), bf16), vm((slots, width), bf16), vm((slots, 1), f32),
            vm((slots, hidden), bf16),
            vm((n_ep, cap, half), bf16), vm((n_ep, cap, half), bf16),
            vm((n_ep, cap, half), bf16), vm((n_ep, cap, half), bf16),
            vm((chips, n_ep, cap, feat), bf16), vm((far, cap, feat), bf16),
            vm((near, cap, half), bf16), vm((far, cap, feat), bf16),
            vm((chips, tok, feat), bf16), vm((chips, tok, feat), bf16),
            sem((2, chips)), sem((2, chips)), sem((2,)), sem((2,)), sem((2,)),
            sem((n_ep,)), sem((n_ep,)), sem((chips, n_ep)), sem((chips, n_ep)),
            sem((n_ep,)), sem((n_ep,)), sem((3,)), sem((3,)),
            sem((chips, n_ep)), sem((chips, n_ep)), sem((n_ep,)), sem((n_ep,)),
            sem((chips,)), sem((chips,)),
            sem((chips,)), sem((chips,)), sem((chips,)), sem((chips,)),
        ]
        a = pl.BlockSpec(memory_space=pl.ANY)
        outs = (
            jax.ShapeDtypeStruct((rows, feat), bf16),
            jax.ShapeDtypeStruct((tok, feat), bf16),
        )
        done = pl.pallas_call(
            functools.partial(kernel, (n_ep, n_tp, cap)),
            out_shape=outs,
            in_specs=[a] * 14,
            out_specs=(a, a),
            scratch_shapes=scratch,
            compiler_params=pltpu.CompilerParams(
                collective_id=0, has_side_effects=True, vmem_limit_bytes=62 << 20
            ),
        )(
            mix_input, mix_gain.reshape(1, -1), gate_b, gate_c, value_w, conv_weight, out_weight,
            expert_input, expert_gain.reshape(1, -1), routes.T, route_weight.T,
            expert_gate, expert_up, expert_down.reshape(hidden, width),
        )
        return pl.pallas_call(
            hand_over,
            out_shape=outs,
            in_specs=[a, a],
            out_specs=(a, a),
            scratch_shapes=[vm((rows, feat), bf16), vm((tok, feat), bf16), sem((2, 2))],
        )(*done)

    in_specs = (
        P("ep", "tp"), P(), P(None, "tp"), P(None, "tp"), P(None, "tp"), P(None, "tp"),
        P("tp", None), P("ep", "tp"), P(), P("ep", None), P("ep", None),
        P("ep", None, "tp"), P("ep", None, "tp"), P("ep", "tp", None),
    )
    out_specs = (P("ep", "tp"), P("ep", "tp"))
    return jax.shard_map(local, mesh=mesh, in_specs=in_specs, out_specs=out_specs, check_vma=False)
```

```python
import functools

import jax
import jax.numpy as jnp
from jax import lax
from jax.experimental import pallas as pl
from jax.experimental.pallas import tpu as pltpu
from jax.sharding import PartitionSpec as P

MESH = pl.DeviceIdType.MESH
epsilon = 1e-06
routed_scale = 2.5
near = 4
f32 = jnp.float32
bf16 = jnp.bfloat16


def kernel(
    dims,
    mix_hbm, mgain_hbm, wb_hbm, wc_hbm, wv_hbm, conv_hbm, wo_hbm,
    exp_hbm, egain_hbm, routes_hbm, rw_hbm, wg_hbm, wu_hbm, wd_hbm,
    mo_hbm, eo_hbm,
    mix_ref, mgain_ref, conv_ref, exp_ref, egain_ref, routes_ref, rw_ref, mo_ref, eo_ref, i_sem,
    wb, wc, wv, wo, wg, wu, wd, w_sem,
    gains, tables, outg,
    xg, xs, fac, outer, prod, edge, gated, pm, om, rm, sm, ym,
    xe, xes, efac, act, pe, oe, re, se, yr, fin, ra, rb, na, ny,
    mys, myr, mps, mpr, edges,
    eps, epr, eys, eyr, pps, ppr, hes, her, ses, ser, rts, rtr, nys, nyr,
    hms, hmr, yms, ymr,
):
    n_ep, n_tp, cap = dims
    chips = n_tp // 2
    n_blk = n_ep // near
    rows, feat = mix_ref.shape
    width = feat * n_tp
    half = feat * chips
    tok = exp_ref.shape[0]
    slots = n_ep * cap
    e = lax.axis_index("ep")
    t = lax.axis_index("tp")
    y, c = lax.div(t, 2), lax.rem(t, 2)
    partner = y * 2 + 1 - c
    blk, idx = lax.div(e, near), lax.rem(e, near)

    def source(p):
        return (
            lax.rem(blk + lax.div(p, near), n_blk) * near
            + lax.rem(idx + lax.rem(p, near), near)
        )

    def target(p):
        return (
            lax.rem(blk - lax.div(p, near) + n_blk, n_blk) * near
            + lax.rem(idx - lax.rem(p, near) + near, near)
        )

    def cols(b):
        return pl.ds(pl.multiple_of(b * feat, feat), feat)

    def lanes(k):
        return cols(c * chips + k)

    own_half = pl.ds(pl.multiple_of(c * half, half), half)

    def remote(src, dst, send_sem, recv_sem, ep, tp):
        return pltpu.make_async_remote_copy(
            src_ref=src, dst_ref=dst, send_sem=send_sem, recv_sem=recv_sem,
            device_id=(ep, tp), device_id_type=MESH,
        )

    def ahead(dy):
        return lax.rem(y + dy, chips)

    def peer(dy):
        return ahead(dy) * 2 + c

    def loop(first, last, body):
        lax.fori_loop(first, last, lambda i, carry: (body(i), carry)[1], 0)

    m_rows = rows // 2

    def mix_y(m, dy):
        at = pl.ds(m * m_rows, m_rows)
        return remote(
            mix_ref.at[at], xg.at[at, lanes(y)], mys.at[m, dy], myr.at[m, dy], e, peer(dy)
        )

    def mix_p(m):
        part = xg.at[pl.ds(m * m_rows, m_rows), own_half]
        return remote(part, part, mps.at[m], mpr.at[m], e, partner)

    def exp_out(p):
        return remote(outg.at[p], xe.at[p, :, lanes(y)], eps.at[p], epr.at[p], target(p), t)

    def exp_y(p, dy):
        part = xe.at[p, :, lanes(y)]
        return remote(part, part, eys.at[dy, p], eyr.at[dy, p], e, peer(dy))

    def exp_p(p):
        part = xe.at[p, :, own_half]
        return remote(part, part, pps.at[p], ppr.at[p], e, partner)

    def edge_copy():
        return remote(
            prod.at[pl.ds(rows, 8)], edge, edges.at[0], edges.at[1], lax.rem(e + 1, n_ep), t
        )

    def exp_half(j, first, last):
        at = pl.ds(first, last - first)
        return remote(pe.at[at], re.at[at], hes.at[j], her.at[j], e, partner)

    def exp_sum(p, dy):
        return remote(
            se.at[p, :, cols(ahead(dy))], yr.at[dy, p], ses.at[dy, p], ser.at[dy, p], e, peer(dy)
        )

    def near_back(p):
        return remote(se.at[p], ra.at[p], rts.at[p], rtr.at[p], source(p), t)

    def far_back(p):
        return remote(
            fin.at[p - near], rb.at[p - near], rts.at[p], rtr.at[p], source(p), t
        )

    def near_sum(dy):
        return remote(na.at[ahead(dy)], ny.at[dy], nys.at[dy], nyr.at[dy], e, peer(dy))

    def mix_half(q):
        return remote(pm.at[q], rm.at[q], hms.at[q], hmr.at[q], e, partner)

    def mix_sum(m, dy):
        at = pl.ds(m * m_rows, m_rows)
        return remote(
            sm.at[dy, at], ym.at[dy, at], yms.at[m, dy], ymr.at[m, dy], e, peer(dy)
        )

    barrier = pltpu.get_barrier_semaphore()
    for dy in range(1, chips):
        pl.semaphore_signal(barrier, inc=1, device_id=(e, peer(dy)), device_id_type=MESH)
    pl.semaphore_signal(barrier, inc=1, device_id=(e, partner), device_id_type=MESH)

    def greet(d):
        pl.semaphore_signal(
            barrier, inc=1, device_id=(lax.rem(e + d, n_ep), t), device_id_type=MESH
        )

    loop(1, n_ep, greet)

    blocks = [(k, (k % chips) * 2 + k // chips) for k in range(n_tp)]

    def turned(src, dst, i):
        return [
            pltpu.make_async_copy(
                src.at[pl.ds(b * feat, feat)], dst.at[pl.ds(k * feat, feat)], w_sem.at[i, k]
            )
            for k, b in blocks
        ]

    loads = {
        "wg": turned(wg_hbm.at[0], wg, 0),
        "wu": turned(wu_hbm.at[0], wu, 1),
        "wd": [pltpu.make_async_copy(wd_hbm, wd, w_sem.at[2, 0])],
        "wc": turned(wc_hbm, wc, 3),
        "wv": turned(wv_hbm, wv, 4),
        "wb": turned(wb_hbm, wb, 5),
        "wo": [pltpu.make_async_copy(wo_hbm, wo, w_sem.at[6, 0])],
    }
    small = {
        name: pltpu.make_async_copy(src, dst, i_sem.at[i])
        for i, (name, src, dst) in enumerate(
            (
                ("routes", routes_hbm, routes_ref), ("exp", exp_hbm, exp_ref),
                ("mix", mix_hbm, mix_ref), ("mgain", mgain_hbm, mgain_ref),
                ("egain", egain_hbm, egain_ref), ("conv", conv_hbm, conv_ref),
                ("rw", rw_hbm, rw_ref),
            )
        )
    }
    for load in small.values():
        load.start()
    for load in small.values():
        load.wait()
    for group in loads.values():
        for load in group:
            load.start()

    def loaded(*names):
        for name in names:
            for load in loads[name]:
                load.wait()

    row = lax.broadcasted_iota(jnp.int32, (tok, tok), 0)
    column = lax.broadcasted_iota(jnp.int32, (tok, tok), 1)

    def upright(line):
        return jnp.sum(jnp.where(row == column, line, 0.0), axis=1, keepdims=True)

    lane_int = lax.broadcasted_iota(jnp.int32, (tok, 128), 1)
    lane = lane_int.astype(f32)
    first_slot = jnp.zeros((1, 128), f32)
    for p in range(n_ep):
        first_slot = first_slot + jnp.where(lane_int[0:1] == target(p), float(p * cap), 0.0)
    named = [upright(routes_ref[k : k + 1, :].astype(f32)) == lane for k in range(2)]
    either = jnp.where(named[0] | named[1], 1.0, 0.0).astype(bf16)
    before = row > column
    counts = jnp.dot(
        jnp.where(before, 1.0, 0.0).astype(bf16), either, preferred_element_type=f32
    )
    places = counts + first_slot
    slot_iota = lax.broadcasted_iota(jnp.int32, (tok, slots), 1).astype(f32)
    both = []
    for k in range(2):
        slot = jnp.sum(jnp.where(named[k], places, 0.0), axis=1, keepdims=True)
        one = jnp.where(slot_iota == slot, 1.0, 0.0)
        tables[k] = one.astype(bf16)
        both.append(one)
    send = (both[0] + both[1]).astype(bf16)

    def select(first, last):
        chosen = send[:, first * cap : last * cap]
        outg[first:last] = (
            lax.dot_general(
                chosen, exp_ref[...], (((0,), (0,)), ((), ())), preferred_element_type=f32
            )
            .astype(bf16)
            .reshape(last - first, cap, feat)
        )

    select(near, n_ep)

    pl.semaphore_wait(barrier, n_ep - 1 + chips)

    middle = near + (n_ep - near) // 2
    parts = [(0, near), (near, middle), (middle, n_ep)]

    def near_send():
        select(0, near)
        loop(1, near, lambda p: exp_out(p).start())
        xe[0, :, lanes(y)] = outg[0]
        for k, b in blocks:
            to, at = pl.ds(k * feat, feat), pl.ds(b * feat, feat)
            gains[0:1, to] = mgain_ref[:, at]
            gains[1:2, to] = egain_ref[:, at]

    def pass_on(p):
        for dy in range(1, chips):
            exp_y(p, dy).start()

    def take(p):
        exp_out(p).wait_recv()
        pass_on(p)

    def relay(p):
        for dy in range(1, chips):
            exp_y(p, dy).wait_recv()
        exp_p(p).start()

    def mix_send(m):
        for dy in range(1, chips):
            mix_y(m, dy).start()

    def mix_sent(m):
        for dy in range(1, chips):
            mix_y(m, dy).wait_send()

    def mix_relay(m):
        for dy in range(1, chips):
            mix_y(m, dy).wait_recv()
        mix_p(m).start()

    def scale_exp(p):
        at = pl.ds(pl.multiple_of(p * cap, cap), cap)
        exp_p(p).wait_recv()
        x = xe[p].astype(f32)
        efac[at] = lax.rsqrt(jnp.sum(x * x, axis=1, keepdims=True) / width + epsilon)
        xes[at] = (x * gains[1:2]).astype(bf16)

    hidden = wd.shape[0]
    wide_h = 256 if hidden % 256 == 0 else hidden

    def scale(j):
        first, last = parts[j]
        loop(first, last, scale_exp)

    def up(j):
        first, last = parts[j]
        part = pl.ds(first * cap, (last - first) * cap)

        def activate(at):
            x = xes[part]
            factor = efac[part]
            gate = jnp.dot(x, wg[:, at], preferred_element_type=f32) * factor
            lift = jnp.dot(x, wu[:, at], preferred_element_type=f32) * factor
            act[part, at] = (gate / (1.0 + jnp.exp(-gate)) * lift).astype(bf16)

        if wide_h == hidden:
            activate(slice(None))
        else:
            loop(
                0, hidden // wide_h,
                lambda i: activate(pl.ds(pl.multiple_of(i * wide_h, wide_h), wide_h)),
            )

    def down(j):
        first, last = parts[j]
        part = pl.ds(first * cap, (last - first) * cap)

        def product(b, into, q):
            out = jnp.dot(act[part], wd[:, cols(b)], preferred_element_type=f32)
            into[pl.ds(first, last - first), :, cols(q)] = out.astype(bf16).reshape(
                last - first, cap, feat
            )

        loop(0, chips, lambda q: product(q * 2 + 1 - c, pe, q))
        exp_half(j, first, last).start()
        loop(0, chips, lambda q: product(q * 2 + c, oe, q))

    def joined(p, at):
        return oe[p, :, at].astype(f32) + re[p, :, at].astype(f32)

    def push_near(p):
        se[p] = joined(p, slice(None)).astype(bf16)

        @pl.when(p > 0)
        def _():
            near_back(p).start()

    def push_far(p):
        for dy in range(1, chips):
            at = cols(ahead(dy))
            se[p, :, at] = joined(p, at).astype(bf16)
            exp_sum(p, dy).start()

    def push(j):
        first, last = parts[j]
        exp_half(j, first, last).wait_recv()
        loop(first, last, push_near if first == 0 else push_far)

    def push_paced(j):
        first, last = parts[j]
        exp_half(j, first, last).wait_recv()
        push_far(first)
        for p in range(first + 1, last):
            for dy in range(1, chips):
                at = cols(ahead(dy))
                se[p, :, at] = joined(p, at).astype(bf16)
            for dy in range(1, chips):
                exp_sum(p - 1, dy).wait_send()
                exp_sum(p, dy).start()

    def finish(p):
        whole = joined(p, cols(y))
        for dy in range(1, chips):
            exp_sum(p, dy).wait_recv()
            whole = whole + yr[dy, p].astype(f32)
        fin[p - near] = whole.astype(bf16)
        far_back(p).start()

    tile = 32

    def scale_mix(i):
        at = pl.ds(pl.multiple_of(i * tile, tile), tile)
        x = xg[at].astype(f32)
        fac[at] = lax.rsqrt(jnp.sum(x * x, axis=1, keepdims=True) / width + epsilon)
        xs[at] = (x * gains[0:1]).astype(bf16)

    wide = 256 if feat % 256 == 0 else feat

    def project(m, i):
        at = pl.ds(pl.multiple_of(i * wide, wide), wide)
        part = pl.ds(m * m_rows, m_rows)
        x = xs[part]
        factor = fac[part]
        inner = jnp.dot(x, wc[:, at], preferred_element_type=f32) * factor
        values = jnp.dot(x, wv[:, at], preferred_element_type=f32) * factor
        prod[pl.ds(8 + m * m_rows, m_rows), at] = inner * values
        outer[part, at] = jnp.dot(x, wb[:, at], preferred_element_type=f32) * factor

    def convolve(i):
        at = pl.ds(pl.multiple_of(i * 128, 128), 128)
        convolved = (
            conv_ref[0:1, at] * prod[pl.ds(6, rows), at]
            + conv_ref[1:2, at] * prod[pl.ds(7, rows), at]
            + conv_ref[2:3, at] * prod[pl.ds(8, rows), at]
        )
        gated[:, at] = (outer[:, at] * convolved).astype(bf16)

    def mix_down(b):
        return jnp.dot(gated[...], wo[:, cols(b)], preferred_element_type=f32).astype(bf16)

    def mix_given(q):
        pm[q] = mix_down(q * 2 + 1 - c)
        mix_half(q).start()

    def mix_kept(q):
        om[q] = mix_down(q * 2 + c)

    def mix_scale(m):
        mix_p(m).wait_recv()
        loop(m * m_rows // tile, (m + 1) * m_rows // tile, scale_mix)

    def mix_gates(m):
        loop(0, feat // wide, lambda i: project(m, i))

    def mix_conv():
        edge_copy().wait_recv()
        prod[0:8] = jnp.where(e == 0, 0.0, edge[...])
        loop(0, feat // 128, convolve)
        loaded("wo")

    def mix_dots():
        loop(0, chips, mix_given)
        loop(0, chips, mix_kept)

    def mix_push(m):
        at = pl.ds(m * m_rows, m_rows)
        if m == 0:
            for q in range(chips):
                mix_half(q).wait_recv()
        for dy in range(1, chips):
            q = ahead(dy)
            sm[dy, at] = (om[q, at].astype(f32) + rm[q, at].astype(f32)).astype(bf16)
            mix_sum(m, dy).start()

    loop(near, middle, lambda p: exp_out(p).start())
    mix_send(0)
    near_send()
    xg[:, lanes(y)] = mix_ref[...]
    mix_sent(0)
    loop(middle, n_ep, lambda p: exp_out(p).start())
    mix_send(1)
    mix_relay(0)
    mix_scale(0)
    loaded("wc", "wv", "wb")
    mix_gates(0)
    loop(near, middle, take)
    mix_relay(1)
    mix_scale(1)
    loop(1, near, take)
    pass_on(0)
    mix_gates(1)
    edge_copy().start()
    loop(near, middle, relay)
    loaded("wg", "wu")
    scale(1)
    up(1)
    loop(middle, n_ep, take)
    loaded("wd")
    down(1)
    mix_conv()
    push(1)
    mix_dots()
    loop(0, near, relay)
    mix_push(0)
    scale(0)
    up(0)
    loop(middle, n_ep, relay)
    down(0)
    loop(near, middle, finish)
    scale(2)
    push(0)
    up(2)
    down(2)
    push(2)
    mix_push(1)
    loop(middle, n_ep, finish)

    scores = rw_ref[...]
    normalized = scores / jnp.sum(scores, axis=0, keepdims=True) * routed_scale
    share = [upright(normalized[k : k + 1, :]) for k in range(2)]

    def combine(first, last, results):
        return share[0] * jnp.dot(
            tables[0, :, first * cap : last * cap], results, preferred_element_type=f32
        ) + share[1] * jnp.dot(
            tables[1, :, first * cap : last * cap], results, preferred_element_type=f32
        )

    ra[0] = se[0]
    loop(1, near, lambda p: near_back(p).wait_recv())
    for q in range(chips):
        at = pl.ds(q * feat, feat)
        na[q] = combine(0, near, ra[:, :, at].reshape(near * cap, feat)).astype(bf16)
    for dy in range(1, chips):
        near_sum(dy).start()

    total = om[y].astype(f32) + rm[y].astype(f32)
    for dy in range(1, chips):
        for m in range(2):
            mix_sum(m, dy).wait_recv()
        total = total + ym[dy].astype(f32)
    mo_ref[...] = total.astype(bf16)
    mo_out = pltpu.make_async_copy(mo_ref, mo_hbm, i_sem.at[7])
    mo_out.start()

    loop(near, n_ep, lambda p: far_back(p).wait_recv())
    result = combine(near, n_ep, rb[...].reshape(slots - near * cap, feat))
    result = result + na[y].astype(f32)
    for dy in range(1, chips):
        near_sum(dy).wait_recv()
        result = result + ny[dy].astype(f32)
    eo_ref[...] = result.astype(bf16)

    eo_out = pltpu.make_async_copy(eo_ref, eo_hbm, i_sem.at[8])
    eo_out.start()
    mo_out.wait()
    eo_out.wait()

    for dy in range(1, chips):
        near_sum(dy).wait_send()
        for m in range(2):
            mix_sum(m, dy).wait_send()
        mix_y(1, dy).wait_send()
    for m in range(2):
        mix_p(m).wait_send()
    edge_copy().wait_send()
    for q in range(chips):
        mix_half(q).wait_send()
    for j, (first, last) in enumerate(parts):
        exp_half(j, first, last).wait_send()

    def drain(p):
        exp_p(p).wait_send()
        for dy in range(1, chips):
            exp_y(p, dy).wait_send()

    def drain_out(p):
        exp_out(p).wait_send()

    def drain_far(p):
        far_back(p).wait_send()

    def drain_sum(p):
        for dy in range(1, chips):
            exp_sum(p, dy).wait_send()

    loop(0, n_ep, drain)
    loop(1, n_ep, drain_out)
    loop(1, near, lambda p: near_back(p).wait_send())
    loop(near, n_ep, drain_far)
    loop(near, n_ep, drain_sum)


def hand_over(mix_hbm, exp_hbm, mo_hbm, eo_hbm, mix_vm, exp_vm, sems):
    pairs = ((exp_hbm, exp_vm, eo_hbm), (mix_hbm, mix_vm, mo_hbm))
    reads = [pltpu.make_async_copy(a, b, sems.at[0, i]) for i, (a, b, _) in enumerate(pairs)]
    writes = [pltpu.make_async_copy(b, d, sems.at[1, i]) for i, (_, b, d) in enumerate(pairs)]
    for read in reads:
        read.start()
    for read, write in zip(reads, writes):
        read.wait()
        write.start()
    for write in writes:
        write.wait()


def solution(mesh):
    n_ep, n_tp = mesh.shape["ep"], mesh.shape["tp"]
    chips = n_tp // 2

    def local(
        mix_input, mix_gain, gate_b, gate_c, value_w, conv_weight, out_weight,
        expert_input, expert_gain, routes, route_weight, expert_gate, expert_up, expert_down,
    ):
        rows, feat = mix_input.shape
        width = feat * n_tp
        half = feat * chips
        tok, top = routes.shape
        experts = n_ep * expert_gate.shape[0]
        assert expert_gate.shape[0] == 1 and top == 2 and n_ep % near == 0
        cap = -(-(2 * tok * top // experts) // 16) * 16
        hidden = expert_gate.shape[2]
        slots = n_ep * cap
        far = n_ep - near
        vm, sem = pltpu.VMEM, pltpu.SemaphoreType.DMA
        scratch = [
            vm((rows, feat), bf16), vm((1, width), f32), vm((3, feat), f32), vm((tok, feat), bf16),
            vm((1, width), f32), vm((2, tok), jnp.int32), vm((2, tok), f32),
            vm((rows, feat), bf16), vm((tok, feat), bf16), sem((9,)),
            vm((width, feat), bf16), vm((width, feat), bf16), vm((width, feat), bf16),
            vm((feat, width), bf16),
            vm((width, hidden), bf16), vm((width, hidden), bf16), vm((hidden, width), bf16),
            sem((7, n_tp)),
            vm((2, width), f32), vm((2, tok, slots), bf16), vm((n_ep, cap, feat), bf16),
            vm((rows, width), bf16), vm((rows, width), bf16), vm((rows, 1), f32),
            vm((rows, feat), f32), vm((rows + 8, feat), f32), vm((8, feat), f32),
            vm((rows, feat), bf16),
            vm((chips, rows, feat), bf16), vm((chips, rows, feat), bf16),
            vm((chips, rows, feat), bf16), vm((chips, rows, feat), bf16),
            vm((chips, rows, feat), bf16),
            vm((n_ep, cap, width), bf16), vm((slots, width), bf16), vm((slots, 1), f32),
            vm((slots, hidden), bf16),
            vm((n_ep, cap, half), bf16), vm((n_ep, cap, half), bf16),
            vm((n_ep, cap, half), bf16), vm((n_ep, cap, half), bf16),
            vm((chips, n_ep, cap, feat), bf16), vm((far, cap, feat), bf16),
            vm((near, cap, half), bf16), vm((far, cap, feat), bf16),
            vm((chips, tok, feat), bf16), vm((chips, tok, feat), bf16),
            sem((2, chips)), sem((2, chips)), sem((2,)), sem((2,)), sem((2,)),
            sem((n_ep,)), sem((n_ep,)), sem((chips, n_ep)), sem((chips, n_ep)),
            sem((n_ep,)), sem((n_ep,)), sem((3,)), sem((3,)),
            sem((chips, n_ep)), sem((chips, n_ep)), sem((n_ep,)), sem((n_ep,)),
            sem((chips,)), sem((chips,)),
            sem((chips,)), sem((chips,)), sem((2, chips)), sem((2, chips)),
        ]
        a = pl.BlockSpec(memory_space=pl.ANY)
        outs = (
            jax.ShapeDtypeStruct((rows, feat), bf16),
            jax.ShapeDtypeStruct((tok, feat), bf16),
        )
        done = pl.pallas_call(
            functools.partial(kernel, (n_ep, n_tp, cap)),
            out_shape=outs,
            in_specs=[a] * 14,
            out_specs=(a, a),
            scratch_shapes=scratch,
            compiler_params=pltpu.CompilerParams(
                collective_id=0, has_side_effects=True, vmem_limit_bytes=62 << 20
            ),
        )(
            mix_input, mix_gain.reshape(1, -1), gate_b, gate_c, value_w, conv_weight, out_weight,
            expert_input, expert_gain.reshape(1, -1), routes.T, route_weight.T,
            expert_gate, expert_up, expert_down.reshape(hidden, width),
        )
        return pl.pallas_call(
            hand_over,
            out_shape=outs,
            in_specs=[a, a],
            out_specs=(a, a),
            scratch_shapes=[vm((rows, feat), bf16), vm((tok, feat), bf16), sem((2, 2))],
        )(*done)

    in_specs = (
        P("ep", "tp"), P(), P(None, "tp"), P(None, "tp"), P(None, "tp"), P(None, "tp"),
        P("tp", None), P("ep", "tp"), P(), P("ep", None), P("ep", None),
        P("ep", None, "tp"), P("ep", None, "tp"), P("ep", "tp", None),
    )
    out_specs = (P("ep", "tp"), P("ep", "tp"))
    return jax.shard_map(local, mesh=mesh, in_specs=in_specs, out_specs=out_specs, check_vma=False)
```

```python
import functools

import jax
import jax.numpy as jnp
from jax import lax
from jax.experimental import pallas as pl
from jax.experimental.pallas import tpu as pltpu
from jax.sharding import PartitionSpec as P

MESH = pl.DeviceIdType.MESH
epsilon = 1e-06
routed_scale = 2.5
near = 4
f32 = jnp.float32
bf16 = jnp.bfloat16


def kernel(
    dims,
    mix_hbm, mgain_hbm, wb_hbm, wc_hbm, wv_hbm, conv_hbm, wo_hbm,
    exp_hbm, egain_hbm, routes_hbm, rw_hbm, wg_hbm, wu_hbm, wd_hbm,
    mo_hbm, eo_hbm,
    mix_ref, mgain_ref, conv_ref, exp_ref, egain_ref, routes_ref, rw_ref, mo_ref, eo_ref, i_sem,
    wb, wc, wv, wo, wg, wu, wd, w_sem,
    gains, tables, outg,
    xg, xs, fac, outer, prod, edge, gated, pm, om, rm, sm, ym,
    xe, xes, efac, act, pe, oe, re, se, yr, fin, ra, rb, na, ny,
    mys, myr, mps, mpr, edges,
    eps, epr, eys, eyr, pps, ppr, hes, her, ses, ser, rts, rtr, nys, nyr,
    hms, hmr, yms, ymr,
):
    n_ep, n_tp, cap = dims
    chips = n_tp // 2
    n_blk = n_ep // near
    rows, feat = mix_ref.shape
    width = feat * n_tp
    half = feat * chips
    tok = exp_ref.shape[0]
    slots = n_ep * cap
    e = lax.axis_index("ep")
    t = lax.axis_index("tp")
    y, c = lax.div(t, 2), lax.rem(t, 2)
    partner = y * 2 + 1 - c
    blk, idx = lax.div(e, near), lax.rem(e, near)

    def source(p):
        return (
            lax.rem(blk + lax.div(p, near), n_blk) * near
            + lax.rem(idx + lax.rem(p, near), near)
        )

    def target(p):
        return (
            lax.rem(blk - lax.div(p, near) + n_blk, n_blk) * near
            + lax.rem(idx - lax.rem(p, near) + near, near)
        )

    def cols(b):
        return pl.ds(pl.multiple_of(b * feat, feat), feat)

    def lanes(k):
        return cols(c * chips + k)

    own_half = pl.ds(pl.multiple_of(c * half, half), half)

    def remote(src, dst, send_sem, recv_sem, ep, tp):
        return pltpu.make_async_remote_copy(
            src_ref=src, dst_ref=dst, send_sem=send_sem, recv_sem=recv_sem,
            device_id=(ep, tp), device_id_type=MESH,
        )

    def ahead(dy):
        return lax.rem(y + dy, chips)

    def peer(dy):
        return ahead(dy) * 2 + c

    def loop(first, last, body):
        lax.fori_loop(first, last, lambda i, carry: (body(i), carry)[1], 0)

    m_rows = rows // 2

    def mix_y(m, dy):
        at = pl.ds(m * m_rows, m_rows)
        return remote(
            mix_ref.at[at], xg.at[at, lanes(y)], mys.at[m, dy], myr.at[m, dy], e, peer(dy)
        )

    def mix_p(m):
        part = xg.at[pl.ds(m * m_rows, m_rows), own_half]
        return remote(part, part, mps.at[m], mpr.at[m], e, partner)

    def exp_out(p):
        return remote(outg.at[p], xe.at[p, :, lanes(y)], eps.at[p], epr.at[p], target(p), t)

    def exp_y(p, dy):
        part = xe.at[p, :, lanes(y)]
        return remote(part, part, eys.at[dy, p], eyr.at[dy, p], e, peer(dy))

    def exp_p(p):
        part = xe.at[p, :, own_half]
        return remote(part, part, pps.at[p], ppr.at[p], e, partner)

    def edge_copy():
        return remote(
            prod.at[pl.ds(rows, 8)], edge, edges.at[0], edges.at[1], lax.rem(e + 1, n_ep), t
        )

    def exp_half(j, first, last):
        at = pl.ds(first, last - first)
        return remote(pe.at[at], re.at[at], hes.at[j], her.at[j], e, partner)

    def exp_sum(p, dy):
        return remote(
            se.at[p, :, cols(ahead(dy))], yr.at[dy, p], ses.at[dy, p], ser.at[dy, p], e, peer(dy)
        )

    def near_back(p):
        return remote(se.at[p], ra.at[p], rts.at[p], rtr.at[p], source(p), t)

    def far_back(p):
        return remote(
            fin.at[p - near], rb.at[p - near], rts.at[p], rtr.at[p], source(p), t
        )

    def near_sum(dy):
        return remote(na.at[ahead(dy)], ny.at[dy], nys.at[dy], nyr.at[dy], e, peer(dy))

    def mix_half(q):
        return remote(pm.at[q], rm.at[q], hms.at[q], hmr.at[q], e, partner)

    def mix_sum(m, dy):
        at = pl.ds(m * m_rows, m_rows)
        return remote(
            sm.at[dy, at], ym.at[dy, at], yms.at[m, dy], ymr.at[m, dy], e, peer(dy)
        )

    barrier = pltpu.get_barrier_semaphore()
    for dy in range(1, chips):
        pl.semaphore_signal(barrier, inc=1, device_id=(e, peer(dy)), device_id_type=MESH)
    pl.semaphore_signal(barrier, inc=1, device_id=(e, partner), device_id_type=MESH)

    def greet(d):
        pl.semaphore_signal(
            barrier, inc=1, device_id=(lax.rem(e + d, n_ep), t), device_id_type=MESH
        )

    loop(1, n_ep, greet)

    blocks = [(k, (k % chips) * 2 + k // chips) for k in range(n_tp)]

    def turned(src, dst, i):
        return [
            pltpu.make_async_copy(
                src.at[pl.ds(b * feat, feat)], dst.at[pl.ds(k * feat, feat)], w_sem.at[i, k]
            )
            for k, b in blocks
        ]

    loads = {
        "wg": turned(wg_hbm.at[0], wg, 0),
        "wu": turned(wu_hbm.at[0], wu, 1),
        "wd": [pltpu.make_async_copy(wd_hbm, wd, w_sem.at[2, 0])],
        "wc": turned(wc_hbm, wc, 3),
        "wv": turned(wv_hbm, wv, 4),
        "wb": turned(wb_hbm, wb, 5),
        "wo": [pltpu.make_async_copy(wo_hbm, wo, w_sem.at[6, 0])],
    }
    small = {
        name: pltpu.make_async_copy(src, dst, i_sem.at[i])
        for i, (name, src, dst) in enumerate(
            (
                ("routes", routes_hbm, routes_ref), ("exp", exp_hbm, exp_ref),
                ("mix", mix_hbm, mix_ref), ("mgain", mgain_hbm, mgain_ref),
                ("egain", egain_hbm, egain_ref), ("conv", conv_hbm, conv_ref),
                ("rw", rw_hbm, rw_ref),
            )
        )
    }
    for load in small.values():
        load.start()
    for load in small.values():
        load.wait()
    for group in loads.values():
        for load in group:
            load.start()

    def loaded(*names):
        for name in names:
            for load in loads[name]:
                load.wait()

    row = lax.broadcasted_iota(jnp.int32, (tok, tok), 0)
    column = lax.broadcasted_iota(jnp.int32, (tok, tok), 1)

    def upright(line):
        return jnp.sum(jnp.where(row == column, line, 0.0), axis=1, keepdims=True)

    lane_int = lax.broadcasted_iota(jnp.int32, (tok, 128), 1)
    lane = lane_int.astype(f32)
    first_slot = jnp.zeros((1, 128), f32)
    for p in range(n_ep):
        first_slot = first_slot + jnp.where(lane_int[0:1] == target(p), float(p * cap), 0.0)
    named = [upright(routes_ref[k : k + 1, :].astype(f32)) == lane for k in range(2)]
    either = jnp.where(named[0] | named[1], 1.0, 0.0).astype(bf16)
    before = row > column
    counts = jnp.dot(
        jnp.where(before, 1.0, 0.0).astype(bf16), either, preferred_element_type=f32
    )
    places = counts + first_slot
    slot_iota = lax.broadcasted_iota(jnp.int32, (tok, slots), 1).astype(f32)
    both = []
    for k in range(2):
        slot = jnp.sum(jnp.where(named[k], places, 0.0), axis=1, keepdims=True)
        one = jnp.where(slot_iota == slot, 1.0, 0.0)
        tables[k] = one.astype(bf16)
        both.append(one)
    send = (both[0] + both[1]).astype(bf16)

    def select(first, last):
        chosen = send[:, first * cap : last * cap]
        outg[first:last] = (
            lax.dot_general(
                chosen, exp_ref[...], (((0,), (0,)), ((), ())), preferred_element_type=f32
            )
            .astype(bf16)
            .reshape(last - first, cap, feat)
        )

    select(near, n_ep)

    pl.semaphore_wait(barrier, n_ep - 1 + chips)

    middle = near + (n_ep - near) // 2
    parts = [(0, near), (near, middle), (middle, n_ep)]

    def near_send():
        select(0, near)
        loop(1, near, lambda p: exp_out(p).start())
        xe[0, :, lanes(y)] = outg[0]
        for k, b in blocks:
            to, at = pl.ds(k * feat, feat), pl.ds(b * feat, feat)
            gains[0:1, to] = mgain_ref[:, at]
            gains[1:2, to] = egain_ref[:, at]

    def pass_on(p):
        for dy in range(1, chips):
            exp_y(p, dy).start()

    def take(p):
        exp_out(p).wait_recv()
        pass_on(p)

    def relay(p):
        for dy in range(1, chips):
            exp_y(p, dy).wait_recv()
        exp_p(p).start()

    def mix_send(m):
        for dy in range(1, chips):
            mix_y(m, dy).start()

    def mix_sent(m):
        for dy in range(1, chips):
            mix_y(m, dy).wait_send()

    def mix_relay(m):
        for dy in range(1, chips):
            mix_y(m, dy).wait_recv()
        mix_p(m).start()

    def scale_exp(p):
        at = pl.ds(pl.multiple_of(p * cap, cap), cap)
        exp_p(p).wait_recv()
        x = xe[p].astype(f32)
        efac[at] = lax.rsqrt(jnp.sum(x * x, axis=1, keepdims=True) / width + epsilon)
        xes[at] = (x * gains[1:2]).astype(bf16)

    hidden = wd.shape[0]
    wide_h = 256 if hidden % 256 == 0 else hidden

    def scale(j):
        first, last = parts[j]
        loop(first, last, scale_exp)

    def up(j):
        first, last = parts[j]
        part = pl.ds(first * cap, (last - first) * cap)

        def activate(at):
            x = xes[part]
            factor = efac[part]
            gate = jnp.dot(x, wg[:, at], preferred_element_type=f32) * factor
            lift = jnp.dot(x, wu[:, at], preferred_element_type=f32) * factor
            act[part, at] = (gate / (1.0 + jnp.exp(-gate)) * lift).astype(bf16)

        if wide_h == hidden:
            activate(slice(None))
        else:
            loop(
                0, hidden // wide_h,
                lambda i: activate(pl.ds(pl.multiple_of(i * wide_h, wide_h), wide_h)),
            )

    def down(j):
        first, last = parts[j]
        part = pl.ds(first * cap, (last - first) * cap)

        def product(b, into, q):
            out = jnp.dot(act[part], wd[:, cols(b)], preferred_element_type=f32)
            into[pl.ds(first, last - first), :, cols(q)] = out.astype(bf16).reshape(
                last - first, cap, feat
            )

        loop(0, chips, lambda q: product(q * 2 + 1 - c, pe, q))
        exp_half(j, first, last).start()
        loop(0, chips, lambda q: product(q * 2 + c, oe, q))

    def joined(p, at):
        return oe[p, :, at].astype(f32) + re[p, :, at].astype(f32)

    def push_near(p):
        se[p] = joined(p, slice(None)).astype(bf16)

        @pl.when(p > 0)
        def _():
            near_back(p).start()

    def push_far(p):
        for dy in range(1, chips):
            at = cols(ahead(dy))
            se[p, :, at] = joined(p, at).astype(bf16)
            exp_sum(p, dy).start()

    def push(j):
        first, last = parts[j]
        exp_half(j, first, last).wait_recv()
        loop(first, last, push_near if first == 0 else push_far)

    def push_paced(j):
        first, last = parts[j]
        exp_half(j, first, last).wait_recv()
        push_far(first)
        for p in range(first + 1, last):
            for dy in range(1, chips):
                at = cols(ahead(dy))
                se[p, :, at] = joined(p, at).astype(bf16)
            for dy in range(1, chips):
                exp_sum(p - 1, dy).wait_send()
                exp_sum(p, dy).start()

    def finish(p):
        whole = joined(p, cols(y))
        for dy in range(1, chips):
            exp_sum(p, dy).wait_recv()
            whole = whole + yr[dy, p].astype(f32)
        fin[p - near] = whole.astype(bf16)
        far_back(p).start()

    tile = 32

    def scale_mix(i):
        at = pl.ds(pl.multiple_of(i * tile, tile), tile)
        x = xg[at].astype(f32)
        fac[at] = lax.rsqrt(jnp.sum(x * x, axis=1, keepdims=True) / width + epsilon)
        xs[at] = (x * gains[0:1]).astype(bf16)

    wide = 256 if feat % 256 == 0 else feat

    def project(m, i):
        at = pl.ds(pl.multiple_of(i * wide, wide), wide)
        part = pl.ds(m * m_rows, m_rows)
        x = xs[part]
        factor = fac[part]
        inner = jnp.dot(x, wc[:, at], preferred_element_type=f32) * factor
        values = jnp.dot(x, wv[:, at], preferred_element_type=f32) * factor
        prod[pl.ds(8 + m * m_rows, m_rows), at] = inner * values
        outer[part, at] = jnp.dot(x, wb[:, at], preferred_element_type=f32) * factor

    def convolve(i):
        at = pl.ds(pl.multiple_of(i * 128, 128), 128)
        convolved = (
            conv_ref[0:1, at] * prod[pl.ds(6, rows), at]
            + conv_ref[1:2, at] * prod[pl.ds(7, rows), at]
            + conv_ref[2:3, at] * prod[pl.ds(8, rows), at]
        )
        gated[:, at] = (outer[:, at] * convolved).astype(bf16)

    def mix_down(b):
        return jnp.dot(gated[...], wo[:, cols(b)], preferred_element_type=f32).astype(bf16)

    def mix_given(q):
        pm[q] = mix_down(q * 2 + 1 - c)
        mix_half(q).start()

    def mix_kept(q):
        om[q] = mix_down(q * 2 + c)

    def mix_scale(m):
        mix_p(m).wait_recv()
        loop(m * m_rows // tile, (m + 1) * m_rows // tile, scale_mix)

    def mix_gates(m):
        loop(0, feat // wide, lambda i: project(m, i))

    def mix_conv():
        edge_copy().wait_recv()
        prod[0:8] = jnp.where(e == 0, 0.0, edge[...])
        loop(0, feat // 128, convolve)
        loaded("wo")

    def mix_dots():
        loop(0, chips, mix_given)
        loop(0, chips, mix_kept)

    def mix_push(m):
        at = pl.ds(m * m_rows, m_rows)
        if m == 0:
            for q in range(chips):
                mix_half(q).wait_recv()
        for dy in range(1, chips):
            q = ahead(dy)
            sm[dy, at] = (om[q, at].astype(f32) + rm[q, at].astype(f32)).astype(bf16)
            mix_sum(m, dy).start()

    loop(near, middle, lambda p: exp_out(p).start())
    mix_send(0)
    near_send()
    xg[:, lanes(y)] = mix_ref[...]
    mix_sent(0)
    loop(middle, n_ep, lambda p: exp_out(p).start())
    mix_send(1)
    mix_relay(0)
    mix_scale(0)
    loaded("wc", "wv", "wb")
    mix_gates(0)
    loop(near, middle, take)
    mix_relay(1)
    mix_scale(1)
    loop(1, near, take)
    pass_on(0)
    mix_gates(1)
    edge_copy().start()
    loop(near, middle, relay)
    loaded("wg", "wu")
    scale(1)
    up(1)
    loaded("wd")
    down(1)
    loop(middle, n_ep, take)
    mix_conv()
    push(1)
    mix_dots()
    loop(0, near, relay)
    scale(0)
    mix_push(0)
    up(0)
    loop(middle, n_ep, relay)
    down(0)
    loop(near, middle, finish)
    scale(2)
    push(0)
    up(2)
    down(2)
    push(2)
    mix_push(1)
    loop(middle, n_ep, finish)

    scores = rw_ref[...]
    normalized = scores / jnp.sum(scores, axis=0, keepdims=True) * routed_scale
    share = [upright(normalized[k : k + 1, :]) for k in range(2)]

    def combine(first, last, results):
        return share[0] * jnp.dot(
            tables[0, :, first * cap : last * cap], results, preferred_element_type=f32
        ) + share[1] * jnp.dot(
            tables[1, :, first * cap : last * cap], results, preferred_element_type=f32
        )

    ra[0] = se[0]
    loop(1, near, lambda p: near_back(p).wait_recv())
    for q in range(chips):
        at = pl.ds(q * feat, feat)
        na[q] = combine(0, near, ra[:, :, at].reshape(near * cap, feat)).astype(bf16)
    for dy in range(1, chips):
        near_sum(dy).start()

    total = om[y].astype(f32) + rm[y].astype(f32)
    for dy in range(1, chips):
        for m in range(2):
            mix_sum(m, dy).wait_recv()
        total = total + ym[dy].astype(f32)
    mo_ref[...] = total.astype(bf16)
    mo_out = pltpu.make_async_copy(mo_ref, mo_hbm, i_sem.at[7])
    mo_out.start()

    loop(near, n_ep, lambda p: far_back(p).wait_recv())
    result = combine(near, n_ep, rb[...].reshape(slots - near * cap, feat))
    result = result + na[y].astype(f32)
    for dy in range(1, chips):
        near_sum(dy).wait_recv()
        result = result + ny[dy].astype(f32)
    eo_ref[...] = result.astype(bf16)

    eo_out = pltpu.make_async_copy(eo_ref, eo_hbm, i_sem.at[8])
    eo_out.start()
    mo_out.wait()
    eo_out.wait()

    for dy in range(1, chips):
        near_sum(dy).wait_send()
        for m in range(2):
            mix_sum(m, dy).wait_send()
        mix_y(1, dy).wait_send()
    for m in range(2):
        mix_p(m).wait_send()
    edge_copy().wait_send()
    for q in range(chips):
        mix_half(q).wait_send()
    for j, (first, last) in enumerate(parts):
        exp_half(j, first, last).wait_send()

    def drain(p):
        exp_p(p).wait_send()
        for dy in range(1, chips):
            exp_y(p, dy).wait_send()

    def drain_out(p):
        exp_out(p).wait_send()

    def drain_far(p):
        far_back(p).wait_send()

    def drain_sum(p):
        for dy in range(1, chips):
            exp_sum(p, dy).wait_send()

    loop(0, n_ep, drain)
    loop(1, n_ep, drain_out)
    loop(1, near, lambda p: near_back(p).wait_send())
    loop(near, n_ep, drain_far)
    loop(near, n_ep, drain_sum)


def hand_over(mix_hbm, exp_hbm, mo_hbm, eo_hbm, mix_vm, exp_vm, sems):
    pairs = ((exp_hbm, exp_vm, eo_hbm), (mix_hbm, mix_vm, mo_hbm))
    reads = [pltpu.make_async_copy(a, b, sems.at[0, i]) for i, (a, b, _) in enumerate(pairs)]
    writes = [pltpu.make_async_copy(b, d, sems.at[1, i]) for i, (_, b, d) in enumerate(pairs)]
    for read in reads:
        read.start()
    for read, write in zip(reads, writes):
        read.wait()
        write.start()
    for write in writes:
        write.wait()


def solution(mesh):
    n_ep, n_tp = mesh.shape["ep"], mesh.shape["tp"]
    chips = n_tp // 2

    def local(
        mix_input, mix_gain, gate_b, gate_c, value_w, conv_weight, out_weight,
        expert_input, expert_gain, routes, route_weight, expert_gate, expert_up, expert_down,
    ):
        rows, feat = mix_input.shape
        width = feat * n_tp
        half = feat * chips
        tok, top = routes.shape
        experts = n_ep * expert_gate.shape[0]
        assert expert_gate.shape[0] == 1 and top == 2 and n_ep % near == 0
        cap = -(-(2 * tok * top // experts) // 16) * 16
        hidden = expert_gate.shape[2]
        slots = n_ep * cap
        far = n_ep - near
        vm, sem = pltpu.VMEM, pltpu.SemaphoreType.DMA
        scratch = [
            vm((rows, feat), bf16), vm((1, width), f32), vm((3, feat), f32), vm((tok, feat), bf16),
            vm((1, width), f32), vm((2, tok), jnp.int32), vm((2, tok), f32),
            vm((rows, feat), bf16), vm((tok, feat), bf16), sem((9,)),
            vm((width, feat), bf16), vm((width, feat), bf16), vm((width, feat), bf16),
            vm((feat, width), bf16),
            vm((width, hidden), bf16), vm((width, hidden), bf16), vm((hidden, width), bf16),
            sem((7, n_tp)),
            vm((2, width), f32), vm((2, tok, slots), bf16), vm((n_ep, cap, feat), bf16),
            vm((rows, width), bf16), vm((rows, width), bf16), vm((rows, 1), f32),
            vm((rows, feat), f32), vm((rows + 8, feat), f32), vm((8, feat), f32),
            vm((rows, feat), bf16),
            vm((chips, rows, feat), bf16), vm((chips, rows, feat), bf16),
            vm((chips, rows, feat), bf16), vm((chips, rows, feat), bf16),
            vm((chips, rows, feat), bf16),
            vm((n_ep, cap, width), bf16), vm((slots, width), bf16), vm((slots, 1), f32),
            vm((slots, hidden), bf16),
            vm((n_ep, cap, half), bf16), vm((n_ep, cap, half), bf16),
            vm((n_ep, cap, half), bf16), vm((n_ep, cap, half), bf16),
            vm((chips, n_ep, cap, feat), bf16), vm((far, cap, feat), bf16),
            vm((near, cap, half), bf16), vm((far, cap, feat), bf16),
            vm((chips, tok, feat), bf16), vm((chips, tok, feat), bf16),
            sem((2, chips)), sem((2, chips)), sem((2,)), sem((2,)), sem((2,)),
            sem((n_ep,)), sem((n_ep,)), sem((chips, n_ep)), sem((chips, n_ep)),
            sem((n_ep,)), sem((n_ep,)), sem((3,)), sem((3,)),
            sem((chips, n_ep)), sem((chips, n_ep)), sem((n_ep,)), sem((n_ep,)),
            sem((chips,)), sem((chips,)),
            sem((chips,)), sem((chips,)), sem((2, chips)), sem((2, chips)),
        ]
        a = pl.BlockSpec(memory_space=pl.ANY)
        outs = (
            jax.ShapeDtypeStruct((rows, feat), bf16),
            jax.ShapeDtypeStruct((tok, feat), bf16),
        )
        done = pl.pallas_call(
            functools.partial(kernel, (n_ep, n_tp, cap)),
            out_shape=outs,
            in_specs=[a] * 14,
            out_specs=(a, a),
            scratch_shapes=scratch,
            compiler_params=pltpu.CompilerParams(
                collective_id=0, has_side_effects=True, vmem_limit_bytes=62 << 20
            ),
        )(
            mix_input, mix_gain.reshape(1, -1), gate_b, gate_c, value_w, conv_weight, out_weight,
            expert_input, expert_gain.reshape(1, -1), routes.T, route_weight.T,
            expert_gate, expert_up, expert_down.reshape(hidden, width),
        )
        return pl.pallas_call(
            hand_over,
            out_shape=outs,
            in_specs=[a, a],
            out_specs=(a, a),
            scratch_shapes=[vm((rows, feat), bf16), vm((tok, feat), bf16), sem((2, 2))],
        )(*done)

    in_specs = (
        P("ep", "tp"), P(), P(None, "tp"), P(None, "tp"), P(None, "tp"), P(None, "tp"),
        P("tp", None), P("ep", "tp"), P(), P("ep", None), P("ep", None),
        P("ep", None, "tp"), P("ep", None, "tp"), P("ep", "tp", None),
    )
    out_specs = (P("ep", "tp"), P("ep", "tp"))
    return jax.shard_map(local, mesh=mesh, in_specs=in_specs, out_specs=out_specs, check_vma=False)
```
